512 devices in a mesh: ep: 32 (over z, x), tp: 16 (over y, core).
Axes of the slice: x: 4, y: 8, z: 8, core: 2. Of those that a mesh axis runs over, the one named last changes fastest.
Arguments:
- mix_rows: bfloat16 [8192, 2048], P('ep'), may hold values from -6 to 6
- mix_gain: bfloat16 [2048], replicated, may hold values from 0.099609375 to 1.8984375
- w_query: bfloat16 [1024, 2048], P('tp'), may hold values from -0.125 to 0.125
- w_key: bfloat16 [1024, 2048], P('tp'), may hold values from -0.125 to 0.125
- w_value: bfloat16 [1024, 2048], P('tp'), may hold values from -0.125 to 0.125
- key_offset: float32 [16, 8192], P('tp'), may hold values from -11 to 0
- w_out: bfloat16 [1024, 2048], P('tp'), may hold values from -0.1875 to 0.1875
- out_gain: bfloat16 [2048], replicated, may hold values from 0.099609375 to 1.8984375
- exp_rows: bfloat16 [3072, 2048], P('ep', 'tp'), may hold values from -100 to 100
- exp_gain: bfloat16 [2048], P('tp'), may hold values from 0.099609375 to 1.8984375
- routes: int32 [3072, 4], P('ep'), may hold values from 0 to 31, all different within a row; in each aligned block of 96 rows (0 to 95, 96 to 191, ...) at most 16 rows name the same one
- route_weight: float32 [3072, 4], P('ep'), may hold values from 0.05 to 1
- w_gate: bfloat16 [32, 2048, 2048], P('ep', None, 'tp'), may hold values from -0.5 to 0.5
- w_up: bfloat16 [32, 2048, 2048], P('ep', None, 'tp'), may hold values from -0.5 to 0.5
- w_down: bfloat16 [32, 2048, 2048], P('ep', 'tp'), may hold values from -0.1875 to 0.1875
Outputs:
- mix_out: bfloat16 [8192, 2048], P('ep')
- exp_out: bfloat16 [3072, 2048], P('ep', 'tp')
The draws below stay inside these ranges and needn't reach their ends.
Inputs may be any that keep to these rules, and one draw needn't show every extreme that they name: `routes`: each row names 4 different experts. Within the rows of one device (aligned blocks of 96 rows) no expert is named by more than 16 rows, and in some blocks one expert is named by exactly 16 rows.
All inputs are finite; a program needn't handle non-finite values.
Results may differ from the reference program's by a relative error of at most 0.019.
Values may be sent and summed in bfloat16 or wider, within the bound.
A program may use at most 128 MiB of HBM per device.

```python
import math
import jax
import jax.numpy as jnp
import numpy as np
from jax import lax

D = 2048
ATTENTION_HEADS = 16
HEAD = 64
FF = 2048
TOPK = 4
MIX_ROWS = 256
EXP_ROWS = 96
EXPERTS = 32
CAP = 16
FF_PART = 128
ATT = 1024
SEQ_LEN = 8192
TOK_B = 3072


def draw_key_offset(key, part):
    starting_key = jax.random.fold_in(key, 101)
    level_key, displacement_key, jitter_key = jax.random.split(starting_key, 3)
    lowest_reach = 0.6
    highest_reach = 1.6
    chain_reach = jax.random.uniform(level_key, (ATTENTION_HEADS, 1), minval=lowest_reach, maxval=highest_reach)
    head_level = jnp.log(chain_reach / SEQ_LEN) - 0.5
    block_shift = jax.random.uniform(displacement_key, (ATTENTION_HEADS, SEQ_LEN // MIX_ROWS), minval=-0.7, maxval=0.7)
    jitter = jax.random.uniform(jitter_key, (ATTENTION_HEADS, SEQ_LEN), minval=-0.5, maxval=0.5)
    offset_values = head_level + jnp.repeat(block_shift, MIX_ROWS, axis=1) + jitter
    return jnp.clip(offset_values, -11.0, 0.0).astype(jnp.float32)


def draw_exp_rows(key, part):
    starting_key = jax.random.fold_in(key, 202)
    noise_key = jax.random.fold_in(starting_key, 0)
    profile = jnp.exp(jnp.linspace(0.0, math.log(6.0), D))[None, :]
    noise = jnp.clip(jax.random.normal(noise_key, (TOK_B, D), jnp.float32), -5.0, 5.0)
    numbers = noise * profile
    return jnp.clip(numbers, -100.0, 100.0).astype(jnp.bfloat16)


def clamp_weights(key, salt):
    starting_key = jax.random.fold_in(key, salt)
    noise_key = jax.random.fold_in(starting_key, 0)
    noise = jnp.clip(jax.random.normal(noise_key, (EXPERTS, D, FF), jnp.float32), -5.0, 5.0) * D ** (-0.5)
    factor = 2.0
    return jnp.clip(noise * factor, -0.5, 0.5).astype(jnp.bfloat16)


def draw_w_gate(key, part):
    return clamp_weights(key, 303)


def draw_w_up(key, part):
    return clamp_weights(key, 404)


def with_spikes(entries, own_key, source, target, shards_of, factor):
    def block_of(position):
        return (jnp.arange(entries.shape[position]) // (entries.shape[position] // shards_of)).reshape((-1,) + (1,) * (entries.ndim - 1 - position))

    first = jax.random.permutation(own_key, shards_of)[block_of(target)]
    other_side = (block_of(target) + shards_of // 2) % shards_of
    return jnp.where((block_of(source) == first) | (block_of(source) == other_side), factor * entries, entries)


def block_scale(rng, extent, cuts, low, high):
    level = 1.0
    for axis_at, shards_of in cuts:
        draws = jax.random.uniform(jax.random.fold_in(jax.random.fold_in(rng, 6), axis_at), (shards_of,), jnp.float32, low / len(cuts), high / len(cuts))
        level = level * jnp.repeat(jnp.exp(draws), extent[axis_at] // shards_of).reshape((-1,) + (1,) * (len(extent) - 1 - axis_at))
    return level


def routed_block(key, own, number, rows, count, top, most, slope):
    ranking = jax.random.permutation(key, count)
    crowded, ordinary = load_shares(count, rows * top, most, slope, True), load_shares(count, rows * top, most, slope, False)
    places = jnp.arange(count)

    def named(sizes, rotation):
        used = int((sizes > 0).sum())
        fixed = max(1, used // 4)
        passed = fixed + (places - fixed + rotation * (used - fixed)) % max(1, count - fixed)
        return jnp.zeros((count,), jnp.int32).at[ranking[jnp.where(places < fixed, places, passed)]].set(jnp.asarray(sizes, jnp.int32))

    sizes = jnp.where(number % 4 == 0, named(crowded, number // 4), named(ordinary, number - number // 4 - 1))
    mixed = jax.random.permutation(jax.random.fold_in(own, 3), count)
    giver, sink = mixed[0:count // 2 * 2:2], mixed[1:count // 2 * 2:2]
    slack = jnp.minimum(sizes[giver] - 1, most - sizes[sink]) // 2
    slack = jnp.where((giver == ranking[0]) | (sink == ranking[0]) | (sizes[sink] == 0), 0, jnp.maximum(slack, 0))
    passed = jax.random.randint(jax.random.fold_in(own, 4), (count // 2,), 0, 1 << 20) % (slack + 1)
    sizes = sizes.at[giver].add(-passed).at[sink].add(passed)
    labels = jnp.searchsorted(jnp.cumsum(sizes), jnp.arange(rows * top), side="right").astype(jnp.int32)
    listing = labels.reshape(top, rows).T
    listing = listing[jax.random.permutation(jax.random.fold_in(own, 1), rows)]
    rotation = jax.random.randint(jax.random.fold_in(own, 2), (rows, 1), 0, top)
    return jnp.take_along_axis(listing, (jnp.arange(top)[None, :] + rotation) % top, axis=1)


def load_shares(amount, total, limit, skew, full):
    portions = [(1 << 20) // math.isqrt(rank ** skew) + 1 for rank in range(1, amount + 1)]
    largest = limit if full else min(limit, max(-(-total // amount), total * portions[0] // sum(portions)))
    least = 1 if total - largest >= amount - 1 else 0
    counts, rest = [largest] + [least] * (amount - 1), total - largest - least * (amount - 1)
    while rest > 0:
        free = [i for i in range(1, amount) if counts[i] < largest] or [i for i in range(1, amount) if counts[i] < limit]
        pool, remaining = sum([portions[i] for i in free]), rest
        for i in free:
            extra = min(limit - counts[i], max(1, remaining * portions[i] // pool), rest)
            counts[i] = counts[i] + extra
            rest = rest - extra
    return np.array(counts)


def bell_draw(own_key, shape, width, reach, shards=(), kind=jnp.bfloat16):
    result = width * jax.random.normal(own_key, shape, jnp.float32)
    if shards:
        result = result * block_scale(own_key, shape, shards, -0.22, 0.18)
    return jnp.clip(result, -reach, reach).astype(kind)


def noise_with(key, extent, spread, reach, cuts, heavy, held_as=jnp.bfloat16):
    array = spread * jax.random.normal(key, extent, jnp.float32)
    if cuts:
        array = array * block_scale(key, extent, cuts, -0.22, 0.18)
    return jnp.clip(with_spikes(array, jax.random.fold_in(key, 3), *heavy), -reach, reach).astype(held_as)


def setup_inputs(seed: int = 0) -> dict:
    arg_keys = jax.random.split(jax.random.key(seed), 16)
    mix_rows = bell_draw(arg_keys[0], (SEQ_LEN, D), 1.0, 6.0, ((0, 32),))
    mix_gain = jnp.clip(1.0 + 0.18 * jax.random.normal(arg_keys[1], (D,), jnp.float32), 0.099609375, 1.8984375).astype(jnp.bfloat16)
    w_query = bell_draw(arg_keys[2], (ATT, D), D ** -0.5, 0.125, ((0, 16),))
    w_key = bell_draw(arg_keys[3], (ATT, D), D ** -0.5, 0.125, ((0, 16),))
    w_value = bell_draw(arg_keys[4], (ATT, D), D ** -0.5, 0.125, ((0, 16),))
    key_offset = draw_key_offset(jax.random.fold_in(arg_keys[15], 71), 0)
    w_out = bell_draw(arg_keys[6], (ATT, D), ATT ** -0.5, 0.1875, ((0, 16),))
    out_gain = jnp.clip(1.0 + 0.18 * jax.random.normal(arg_keys[7], (D,), jnp.float32), 0.099609375, 1.8984375).astype(jnp.bfloat16)
    exp_rows = draw_exp_rows(jax.random.fold_in(arg_keys[15], 71), 0)
    exp_gain = jnp.clip(1.0 + 0.18 * jax.random.normal(arg_keys[9], (D,), jnp.float32), 0.099609375, 1.8984375).astype(jnp.bfloat16)
    routes_keys = jax.random.split(jax.random.fold_in(arg_keys[10], 1), TOK_B // EXP_ROWS)
    routes_turns = jax.random.permutation(jax.random.fold_in(arg_keys[10], 3), TOK_B // EXP_ROWS)
    routes = jax.vmap(lambda own, number: routed_block(jax.random.fold_in(arg_keys[10], 2), own, number, EXP_ROWS, EXPERTS, TOPK, CAP, 1))(routes_keys, routes_turns).reshape((TOK_B, TOPK))
    route_weight = jnp.clip(jnp.exp(math.log(1.0) - 2.9957323 * jax.random.uniform(arg_keys[11], (TOK_B, TOPK), jnp.float32) ** block_scale(arg_keys[11], (TOK_B, TOPK), ((0, 32),), -0.2, 0.2)), 0.05, 1.0)
    w_gate = draw_w_gate(jax.random.fold_in(arg_keys[15], 71), 0)
    w_up = draw_w_up(jax.random.fold_in(arg_keys[15], 71), 0)
    w_down = noise_with(arg_keys[14], (EXPERTS, FF, D), FF ** -0.5, 0.1875, ((0, 32), (1, 16)), (1, 2, 16, 2.0))
    return {"mix_rows": mix_rows, "mix_gain": mix_gain, "w_query": w_query, "w_key": w_key, "w_value": w_value, "key_offset": key_offset, "w_out": w_out, "out_gain": out_gain, "exp_rows": exp_rows, "exp_gain": exp_gain, "routes": routes, "route_weight": route_weight, "w_gate": w_gate, "w_up": w_up, "w_down": w_down}


EPSILON = 1e-06
CLAMP_LIMIT = 7.0
SILU_SHARPNESS = 1.702

def normalize(matrix, gain):
    numbers = matrix.astype(jnp.float32)
    factor = lax.rsqrt(lax.optimization_barrier(jnp.mean(numbers * numbers, axis=-1, keepdims=True)) + EPSILON)
    return numbers * factor * gain.astype(jnp.float32)

def project(normed, weight):
    product = lax.dot_general(normed, weight, (((1,), (1,)), ((), ())), preferred_element_type=jnp.float32)
    return product.astype(jnp.bfloat16)

def stick_weights(scores, visible):
    keep_log = jnp.where(visible, jax.nn.log_sigmoid(-scores), 0.0)
    later_sum = lax.cumsum(keep_log, axis=2, reverse=True) - keep_log
    return jnp.where(visible, jnp.exp(jax.nn.log_sigmoid(scores) + later_sum), 0.0)

def gated_units(gate_pre, up_pre):
    gate_part = jnp.minimum(gate_pre, CLAMP_LIMIT)
    up_part = jnp.clip(up_pre, -CLAMP_LIMIT, CLAMP_LIMIT)
    return (up_part + 1.0) * (gate_part * jax.nn.sigmoid(SILU_SHARPNESS * gate_part))

def reference(mix_rows, mix_gain, w_query, w_key, w_value, key_offset, w_out, out_gain, exp_rows, exp_gain, routes, route_weight, w_gate, w_up, w_down):
    normed = normalize(mix_rows, mix_gain).astype(jnp.bfloat16)
    length = normed.shape[0]
    queries = project(normed, w_query).astype(jnp.float32).reshape(length, ATTENTION_HEADS, HEAD)
    key_rows = project(normed, w_key).astype(jnp.float32).reshape(length, ATTENTION_HEADS, HEAD)
    value_rows = project(normed, w_value).astype(jnp.float32).reshape(length, ATTENTION_HEADS, HEAD)
    offset_values = key_offset.astype(jnp.float32)
    key_index = jnp.arange(length, dtype=jnp.int32)

    def one_block(first_row):
        block_q = lax.dynamic_slice_in_dim(queries, first_row, MIX_ROWS, 0)
        scores = jnp.einsum('thd,shd->hts', block_q, key_rows) / math.sqrt(HEAD) + offset_values[:, None, :]
        query_index = first_row + jnp.arange(MIX_ROWS, dtype=jnp.int32)
        visible = (key_index[None, :] < query_index[:, None])[None]
        weights = stick_weights(scores, visible).astype(jnp.bfloat16)
        weights = lax.optimization_barrier(weights).astype(jnp.float32)
        return jnp.einsum('hts,shd->thd', weights, value_rows)
    starts = jnp.arange(length // MIX_ROWS, dtype=jnp.int32) * MIX_ROWS
    attended = lax.map(one_block, starts).reshape(length, ATTENTION_HEADS * HEAD).astype(jnp.bfloat16)
    mixed_sum = jnp.dot(attended, w_out, preferred_element_type=jnp.float32)
    mix_out = normalize(mixed_sum, out_gain).astype(jnp.bfloat16)
    tokens = exp_rows.shape[0]
    normed_exp = normalize(exp_rows, exp_gain).astype(jnp.bfloat16)
    route_list = routes.reshape(-1).astype(jnp.int32)
    pair_count = route_list.shape[0]
    owners = jnp.arange(pair_count, dtype=jnp.int32) // TOPK
    block_of = owners // EXP_ROWS
    matches = (route_list[:, None] == jnp.arange(EXPERTS, dtype=jnp.int32)[None, :]).astype(jnp.int32)
    grouped = matches.reshape(tokens // EXP_ROWS, EXP_ROWS * TOPK, EXPERTS)
    earlier = (jnp.cumsum(grouped, axis=1) - grouped).reshape(pair_count, EXPERTS)
    slot_index = block_of * CAP + lax.optimization_barrier(jnp.sum(earlier * matches, axis=1))
    table = jnp.full((EXPERTS, tokens // EXP_ROWS * CAP), -1, jnp.int32).at[route_list, slot_index].set(owners)
    piece_count = FF // FF_PART

    def one_expert(operands):
        chosen, gate_weight, up_weight, down_weight = operands
        expert_rows = jnp.where(chosen[:, None] >= 0, normed_exp[jnp.maximum(chosen, 0)], jnp.zeros((), jnp.bfloat16))
        gate_pre = jnp.dot(expert_rows, gate_weight, preferred_element_type=jnp.float32)
        up_pre = jnp.dot(expert_rows, up_weight, preferred_element_type=jnp.float32)
        hidden = gated_units(gate_pre, up_pre).astype(jnp.bfloat16)
        row_total = hidden.shape[0]
        partials = jnp.einsum('spw,pwd->psd', hidden.astype(jnp.float32).reshape(row_total, piece_count, FF_PART), down_weight.astype(jnp.float32).reshape(piece_count, FF_PART, D))
        partials = lax.optimization_barrier(partials.astype(jnp.bfloat16)).astype(jnp.float32)
        return lax.optimization_barrier(jnp.sum(partials, axis=0)).astype(jnp.bfloat16)
    expert_out = lax.map(one_expert, (table, w_gate, w_up, w_down))
    picked = expert_out[route_list, slot_index].astype(jnp.float32).reshape(tokens, TOPK, D)
    exp_out = lax.optimization_barrier(jnp.sum(picked * route_weight.astype(jnp.float32)[:, :, None], axis=1)).astype(jnp.bfloat16)
    return (mix_out, exp_out)
```

```python
import math

import jax
import jax.numpy as jnp
from jax import lax
from jax.experimental import pallas as pl
from jax.experimental.pallas import tpu as pltpu
from jax.sharding import Mesh
from jax.sharding import PartitionSpec as P

EP = ("ep_0", "ep_1")
TP = ("tp_0", "tp_1")
Z, X, Y, C = 8, 4, 8, 2
N_EP, N_TP = Z * X, Y * C

EPSILON = 1e-06
CLAMP_LIMIT = 7.0
SILU_SHARPNESS = 1.702
LOG2E = math.log2(math.e)

D = 2048
HEAD = 64
ROWS = 256
HALF = ROWS // 2
TOK = 96
CAP = 16
SLOTS = N_EP * CAP
COLS = D // N_TP
GAIN_ROWS = 16

F32 = jnp.float32
BF16 = jnp.bfloat16
MESH = pl.DeviceIdType.MESH
NT = (((1,), (1,)), ((), ()))
TN = (((0,), (0,)), ((), ()))


def dot(a, b):
    return jnp.dot(a, b, preferred_element_type=F32)


def iota(shape, dim):
    return lax.broadcasted_iota(jnp.int32, shape, dim)


def split_two(value):
    high = value.astype(BF16)
    return high, (value - high.astype(F32)).astype(BF16)


def body(
    mix_rows, mix_gain, w_query, w_key, w_value, key_offset, w_out, out_gain, exp_rows, exp_gain,
    routes, route_weight, w_gate, w_up, w_down,
    mix_out, exp_out,
    rows, wqkv, q_pad, kvg, acc, carry, tri,
    picks, weight_hi, weight_lo, sent, grid, wgu, gu, ssq, hid, wd_own, wd, wo_own, wo,
    att, out_acc, cols, result, returned,
    load_sem, disp_send, disp_recv, kva_send, kva_recv, kvb_send, kvb_recv,
    grid_send, grid_recv, hid_send, hid_recv, wd_send, wd_recv, wo_send, wo_recv,
    att_send, att_recv, cols_send, cols_recv, ret_send, ret_recv,
):
    z, x = lax.axis_index("ep_0"), lax.axis_index("ep_1")
    y, c = lax.axis_index("tp_0"), lax.axis_index("tp_1")
    ep, tp = z * X + x, y * C + c
    partner = {"tp_1": 1 - c}
    y_up, y_down = {"tp_0": lax.rem(y + 1, Y)}, {"tp_0": lax.rem(y + Y - 1, Y)}
    z_up, z_down = {"ep_0": lax.rem(z + 1, Z)}, {"ep_0": lax.rem(z + Z - 1, Z)}

    def ep_peer(distance):
        other = lax.rem(ep + distance, N_EP)
        return other, {"ep_0": other // X, "ep_1": lax.rem(other, X)}

    def tp_peer(distance):
        other = lax.rem(tp + distance, N_TP)
        return other, {"tp_0": other // C, "tp_1": lax.rem(other, C)}

    def remote(src, dst, send_sem, recv_sem, device):
        return pltpu.make_async_remote_copy(
            src_ref=src, dst_ref=dst, send_sem=send_sem, recv_sem=recv_sem,
            device_id=device, device_id_type=MESH,
        )

    loads = [
        (mix_rows, rows),
        (w_query, wqkv.at[pl.ds(0, HEAD)]),
        (w_key, wqkv.at[pl.ds(2 * HEAD, HEAD)]),
        (w_value, wqkv.at[pl.ds(3 * HEAD, HEAD)]),
        (w_out, wo_own),
        (w_down.at[0], wd_own),
        (w_gate.at[0], wgu.at[:, pl.ds(0, COLS)]),
        (w_up.at[0], wgu.at[:, pl.ds(COLS, COLS)]),
    ]
    loads = [pltpu.make_async_copy(a, b, load_sem.at[n]) for n, (a, b) in enumerate(loads)]
    for load in loads:
        load.start()

    barrier = pltpu.get_barrier_semaphore()

    @pl.loop(1, N_EP)
    def _(distance):
        pl.semaphore_signal(barrier, 1, device_id=ep_peer(distance)[1], device_id_type=MESH)

    @pl.loop(1, N_TP)
    def _(distance):
        pl.semaphore_signal(barrier, 1, device_id=tp_peer(distance)[1], device_id_type=MESH)

    lane = iota((TOK, 128), 1)
    member = jnp.zeros((TOK, 128), F32)
    weight = jnp.zeros((TOK, 128), F32)
    for k in range(routes.shape[1]):
        hit = routes[:, k : k + 1] == lane
        member = member + jnp.where(hit, 1.0, 0.0)
        weight = weight + jnp.where(hit, route_weight[:, k : k + 1], 0.0)
    member = member.astype(BF16)
    earlier = jnp.where(iota((TOK, TOK), 1) < iota((TOK, TOK), 0), 1.0, 0.0).astype(BF16)
    before = dot(earlier, member).astype(BF16)
    spread = jnp.where(iota((128, SLOTS), 1) // CAP == iota((128, SLOTS), 0), 1.0, 0.0).astype(BF16)
    place = lax.rem(iota((TOK, SLOTS), 1), CAP).astype(F32)
    chosen = (dot(member, spread) > 0.5) & (dot(before, spread) == place)
    picks[...] = jnp.where(chosen, 1.0, 0.0).astype(BF16)
    high, low = split_two(weight)
    weight_hi[...] = jnp.where(chosen, dot(high, spread), 0.0).astype(BF16)
    weight_lo[...] = jnp.where(chosen, dot(low, spread), 0.0).astype(BF16)
    sent[...] = lax.dot_general(picks[...], exp_rows[...], TN, preferred_element_type=F32).astype(BF16)
    own_slots = pl.ds(pl.multiple_of(ep * CAP, CAP), CAP)
    grid[tp, own_slots, :] = sent[own_slots, :]
    grid[tp, pl.ds(SLOTS, GAIN_ROWS), :] = jnp.broadcast_to(exp_gain[...], (GAIN_ROWS, COLS))

    wqkv[pl.ds(HEAD, HEAD), :] = jnp.zeros((HEAD, D), BF16)
    tri[...] = jnp.where(
        (iota((256, 256), 1) >= HALF)
        | (lax.rem(iota((256, 256), 0), HALF) >= iota((256, 256), 1)), 1.0, 0.0,
    ).astype(BF16)
    loads[0].wait()
    gain = mix_gain[...].astype(F32)

    @pl.loop(0, ROWS // 32)
    def _(n):
        at = pl.ds(pl.multiple_of(n * 32, 32), 32)
        numbers = rows[at, :].astype(F32)
        factor = lax.rsqrt(jnp.mean(numbers * numbers, axis=-1, keepdims=True) + EPSILON)
        rows[at, :] = (numbers * factor * gain).astype(BF16)

    for load in loads[1:4]:
        load.wait()
    projected = lax.dot_general(rows[...], wqkv[...], NT, preferred_element_type=F32).astype(BF16)
    q_pad[...] = projected[:, : 2 * HEAD]
    kvg[ep] = projected[:, 2 * HEAD :]
    loads[4].wait()
    loads[5].wait()

    pl.semaphore_wait(barrier, N_EP - 1 + N_TP - 1)

    part_a, part_b = pl.ds(0, HALF), pl.ds(HALF, HALF)

    def send_a(slot, device):
        part = kvg.at[slot, part_a]
        remote(part, part, kva_send, kva_recv.at[slot], device).start()

    def send_b(slot, device):
        part = kvg.at[slot, part_b]
        remote(part, part, kvb_send, kvb_recv.at[slot], device).start()

    def wait_a(slot):
        part = kvg.at[slot, part_a]
        remote(part, part, kva_send, kva_recv.at[slot], partner).wait_recv()

    def wait_b(slot):
        part = kvg.at[slot, part_b]
        remote(part, part, kvb_send, kvb_recv.at[slot], partner).wait_recv()

    def x_peer(distance):
        return lax.rem(x + distance, X)

    def send_b_across(slot):
        for distance in range(1, X):
            send_b(slot, {"ep_1": x_peer(distance)})

    def disp_copy(distance):
        other, device = ep_peer(distance)
        return remote(
            sent.at[pl.ds(pl.multiple_of(other * CAP, CAP), CAP)],
            grid.at[tp, own_slots],
            disp_send, disp_recv, device,
        )

    @pl.loop(1, N_EP)
    def _(distance):
        disp_copy(distance).start()

    for distance in range(1, X):
        send_a(ep, {"ep_1": x_peer(distance)})
    send_b(ep, z_up)
    send_b(ep, z_down)
    send_a(ep, z_up)
    send_a(ep, z_down)
    send_b_across(ep)

    def columns_of(other):
        return pl.ds(pl.multiple_of(other * COLS, COLS), COLS)

    own_columns = columns_of(tp)

    @pl.loop(1, N_TP)
    def _(distance):
        other, device = tp_peer(distance)
        remote(wd_own.at[:, columns_of(other)], wd.at[tp], wd_send, wd_recv, device).start()

    @pl.loop(1, N_TP)
    def _(distance):
        other, device = tp_peer(distance)
        remote(wo_own.at[:, columns_of(other)], wo.at[tp], wo_send, wo_recv, device).start()

    wd[tp] = wd_own[:, own_columns]
    wo[tp] = wo_own[:, own_columns]

    for distance in range(1, X):
        slot = z * X + x_peer(distance)
        wait_a(slot)
        send_a(slot, z_up)
        send_a(slot, z_down)

    def attend(block, diagonal):
        kv = kvg[block]
        offsets = key_offset[:, pl.ds(pl.multiple_of(block * ROWS, ROWS), ROWS)] * LOG2E
        scores = lax.dot_general(q_pad[...], kv, NT, preferred_element_type=F32)
        scores = scores * (LOG2E / math.sqrt(HEAD)) + offsets
        drop = jnp.maximum(jnp.log2(1.0 + jnp.exp2(jnp.minimum(scores, 100.0))), scores)
        if diagonal:
            visible = iota((ROWS, ROWS), 1) < iota((ROWS, ROWS), 0)
            drop = jnp.where(visible, drop, 0.0)
        for half in (1, 0):
            at = slice(half * HALF, (half + 1) * HALF)
            totals = dot(jnp.concatenate(split_two(drop[:, at]), axis=1), tri[...])
            weights = jnp.exp2(scores[:, at] - totals[:, :HALF] - carry[...])
            if diagonal:
                weights = jnp.where(visible[:, at], weights, 0.0)
            acc[...] += dot(weights.astype(BF16), kv[at, :])
            carry[...] += totals[:, HALF:]

    def attend_row(back):
        row = z - back

        @pl.when(row >= 0)
        def _():
            @pl.loop(0, X)
            def _(n):
                attend(row * X + X - 1 - n, False)

    acc[...] = jnp.zeros(acc.shape, F32)
    carry[...] = jnp.zeros(carry.shape, F32)
    attend(ep, True)
    for distance in range(1, X):
        wait_b(z * X + x_peer(distance))

    @pl.loop(0, x)
    def _(n):
        attend(ep - 1 - n, False)

    def ring(buffer, send_sem, recv_sem):
        def send(slot, device):
            block = buffer.at[slot]
            remote(block, block, send_sem, recv_sem.at[slot], device).start()

        def wait(slot):
            block = buffer.at[slot]
            remote(block, block, send_sem, recv_sem.at[slot], partner).wait_recv()

        def start():
            for device in (y_up, y_down, partner):
                send(tp, device)

        def step(k):
            slot = lax.rem(y + Y - k, Y) * C + c
            wait(slot)
            if k < Y // 2:
                send(slot, y_up)
            send(slot, partner)
            if k < Y // 2:
                slot = lax.rem(y + k, Y) * C + c
                wait(slot)
                if k < Y // 2 - 1:
                    send(slot, y_down)
                send(slot, partner)

        def finish():
            @pl.loop(0, Y)
            def _(n):
                wait(n * C + 1 - c)

        def drain():
            blocks = buffer.at[pl.ds(0, N_TP - 1)]
            remote(blocks, blocks, send_sem, recv_sem.at[0], partner).wait_send()

        return start, step, finish, drain

    grid_ring = ring(grid, grid_send, grid_recv)
    hid_ring = ring(hid, hid_send, hid_recv)
    att_ring = ring(att, att_send, att_recv)
    cols_ring = ring(cols, cols_send, cols_recv)

    arrived = grid.at[tp, pl.ds(0, SLOTS - CAP)]
    remote(arrived, arrived, disp_send, disp_recv, partner).wait_recv()
    grid_ring[0]()

    def kv_step(k):
        row = lax.rem(z + Z - k, Z) * X
        for distance in range(X):
            slot = row + x_peer(distance)
            wait_a(slot)
            if k < Z // 2:
                send_a(slot, z_up)
        slot = row + x
        wait_b(slot)
        if k < Z // 2:
            send_b(slot, z_up)
        send_b_across(slot)
        if k < Z // 2:
            row = lax.rem(z + k, Z) * X
            for distance in range(X):
                slot = row + x_peer(distance)
                wait_a(slot)
                if k < Z // 2 - 1:
                    send_a(slot, z_down)
            slot = row + x
            wait_b(slot)
            if k < Z // 2 - 1:
                send_b(slot, z_down)
            send_b_across(slot)

    def kv_finish(k):
        row = lax.rem(z + Z - k, Z) * X
        for distance in range(1, X):
            wait_b(row + x_peer(distance))

    for k in range(1, 5):
        kv_step(k)
        grid_ring[1](k)
        if k > 1:
            kv_finish(k - 1)
            attend_row(k - 1)

    grid_ring[2]()
    loads[6].wait()
    loads[7].wait()
    gu[...] = jnp.zeros(gu.shape, F32)
    ssq[...] = jnp.zeros(ssq.shape, F32)

    @pl.loop(0, N_TP // 2)
    def _(n):
        scaled = []
        for m in range(2):
            numbers = grid[2 * n + m, pl.ds(0, SLOTS), :].astype(F32)
            gains = grid[2 * n + m, pl.ds(SLOTS, GAIN_ROWS), :][:1].astype(F32)
            ssq[...] += numbers * numbers
            scaled.append((numbers * gains).astype(BF16))
        part = wgu[pl.ds(pl.multiple_of(n * 2 * COLS, 2 * COLS), 2 * COLS), :]
        gu[...] += dot(jnp.concatenate(scaled, axis=1), part)

    factor = lax.rsqrt(jnp.sum(ssq[...], axis=1, keepdims=True) / D + EPSILON)
    gate_part = jnp.minimum(gu[:, :COLS] * factor, CLAMP_LIMIT)
    up_part = jnp.clip(gu[:, COLS:] * factor, -CLAMP_LIMIT, CLAMP_LIMIT)
    hid[tp] = (
        (up_part + 1.0) * (gate_part * jax.nn.sigmoid(SILU_SHARPNESS * gate_part))
    ).astype(BF16)
    hid_ring[0]()

    for k in range(4, 8):
        kv_finish(k)
        attend_row(k)
    first = pltpu.roll(acc[pl.ds(0, HALF), :], HEAD, 1)
    att[tp] = jnp.where(iota((HALF, 128), 1) < HEAD, first, acc[pl.ds(HALF, HALF), :]).astype(BF16)
    att_ring[0]()
    for k in range(1, 5):
        att_ring[1](k)
        hid_ring[1](k)
    att_ring[2]()

    pieces = wo.at[pl.ds(0, N_TP - 1)]
    remote(pieces, pieces, wo_send, wo_recv, partner).wait_recv()
    out_acc[...] = jnp.zeros(out_acc.shape, F32)

    @pl.loop(0, N_TP)
    def _(n):
        piece = wo[n]
        zeros = jnp.zeros_like(piece)
        twice = jnp.concatenate(
            [jnp.concatenate([piece, zeros], axis=1), jnp.concatenate([zeros, piece], axis=1)], axis=0
        )
        out_acc[...] += dot(att[n], twice)

    cols[tp, pl.ds(0, HALF), :] = out_acc[:, :COLS].astype(BF16)
    cols[tp, pl.ds(HALF, HALF), :] = out_acc[:, COLS:].astype(BF16)
    cols_ring[0]()

    hid_ring[2]()
    pieces = wd.at[pl.ds(0, N_TP - 1)]
    remote(pieces, pieces, wd_send, wd_recv, partner).wait_recv()
    gu[:, :COLS] = jnp.zeros((SLOTS, COLS), F32)

    @pl.loop(0, N_TP // 2)
    def _(n):
        left = jnp.concatenate([hid[2 * n], hid[2 * n + 1]], axis=1)
        right = jnp.concatenate([wd[2 * n], wd[2 * n + 1]], axis=0)
        gu[:, :COLS] += dot(left, right)

    result[...] = gu[:, :COLS].astype(BF16)
    returned[own_slots, :] = result[own_slots, :]

    @pl.loop(1, N_EP)
    def _(distance):
        other, device = ep_peer(distance)
        remote(
            result.at[pl.ds(pl.multiple_of(other * CAP, CAP), CAP)],
            returned.at[own_slots],
            ret_send, ret_recv, device,
        ).start()

    for k in range(1, 5):
        cols_ring[1](k)
    cols_ring[2]()

    squares = jnp.zeros((ROWS, COLS), F32)
    for n in range(N_TP):
        numbers = cols[n].astype(F32)
        squares = squares + numbers * numbers
    factor = lax.rsqrt(jnp.sum(squares, axis=1, keepdims=True) / D + EPSILON)
    for n in range(N_TP):
        at = slice(n * COLS, (n + 1) * COLS)
        mix_out[:, at] = (cols[n].astype(F32) * factor * out_gain[:, at].astype(F32)).astype(BF16)

    arrived = returned.at[pl.ds(0, SLOTS - CAP)]
    remote(arrived, arrived, ret_send, ret_recv, partner).wait_recv()
    exp_out[...] = (dot(weight_hi[...], returned[...]) + dot(weight_lo[...], returned[...])).astype(BF16)

    part = kvg.at[pl.ds(0, N_EP - 1), part_a]
    remote(part, part, kva_send, kva_recv.at[0], partner).wait_send()
    remote(part, part, kvb_send, kvb_recv.at[0], partner).wait_send()
    part = sent.at[pl.ds(0, SLOTS - CAP)]
    remote(part, part, disp_send, disp_recv, partner).wait_send()
    remote(part, part, ret_send, ret_recv, partner).wait_send()
    part = wd.at[pl.ds(0, N_TP - 1)]
    remote(part, part, wd_send, wd_recv, partner).wait_send()
    part = wo.at[pl.ds(0, N_TP - 1)]
    remote(part, part, wo_send, wo_recv, partner).wait_send()
    for one in (grid_ring, hid_ring, att_ring, cols_ring):
        one[3]()


def on_device(*args):
    (mix_rows, mix_gain, w_query, w_key, w_value, key_offset, w_out, out_gain, exp_rows, exp_gain,
     routes, route_weight, w_gate, w_up, w_down) = args
    vmem, hbm = pl.BlockSpec(memory_space=pltpu.VMEM), pl.BlockSpec(memory_space=pl.ANY)
    dma = pltpu.SemaphoreType.DMA
    return pl.pallas_call(
        body,
        out_shape=(
            jax.ShapeDtypeStruct((ROWS, D), BF16),
            jax.ShapeDtypeStruct((TOK, COLS), BF16),
        ),
        in_specs=[
            hbm, vmem, hbm, hbm, hbm, vmem, hbm, vmem, vmem, vmem, vmem, vmem, hbm, hbm, hbm,
        ],
        out_specs=(vmem, vmem),
        scratch_shapes=[
            pltpu.VMEM((ROWS, D), BF16),
            pltpu.VMEM((4 * HEAD, D), BF16),
            pltpu.VMEM((ROWS, 128), BF16),
            pltpu.VMEM((N_EP, ROWS, 128), BF16),
            pltpu.VMEM((ROWS, 128), F32),
            pltpu.VMEM((ROWS, 128), F32),
            pltpu.VMEM((256, 256), BF16),
            pltpu.VMEM((TOK, SLOTS), BF16),
            pltpu.VMEM((TOK, SLOTS), BF16),
            pltpu.VMEM((TOK, SLOTS), BF16),
            pltpu.VMEM((SLOTS, COLS), BF16),
            pltpu.VMEM((N_TP, SLOTS + GAIN_ROWS, COLS), BF16),
            pltpu.VMEM((D, 2 * COLS), BF16),
            pltpu.VMEM((SLOTS, 2 * COLS), F32),
            pltpu.VMEM((SLOTS, COLS), F32),
            pltpu.VMEM((N_TP, SLOTS, COLS), BF16),
            pltpu.VMEM((COLS, D), BF16),
            pltpu.VMEM((N_TP, COLS, COLS), BF16),
            pltpu.VMEM((HEAD, D), BF16),
            pltpu.VMEM((N_TP, HEAD, COLS), BF16),
            pltpu.VMEM((N_TP, HALF, 128), BF16),
            pltpu.VMEM((HALF, 2 * COLS), F32),
            pltpu.VMEM((N_TP, ROWS, COLS), BF16),
            pltpu.VMEM((SLOTS, COLS), BF16),
            pltpu.VMEM((SLOTS, COLS), BF16),
            dma((8,)),
            dma(()), dma(()),
            dma(()), dma((N_EP,)), dma(()), dma((N_EP,)),
            dma(()), dma((N_TP,)), dma(()), dma((N_TP,)),
            dma(()), dma(()), dma(()), dma(()),
            dma(()), dma((N_TP,)), dma(()), dma((N_TP,)),
            dma(()), dma(()),
        ],
        compiler_params=pltpu.CompilerParams(
            collective_id=0, has_side_effects=True, vmem_limit_bytes=60 * 1024 * 1024
        ),
    )(
        mix_rows, mix_gain.reshape(1, D), w_query, w_key, w_value, key_offset, w_out,
        out_gain.reshape(1, D), exp_rows, exp_gain.reshape(1, COLS), routes, route_weight,
        w_gate, w_up, w_down,
    )


def solution(mesh):
    torus = Mesh(mesh.devices.reshape(Z, X, Y, C), EP + TP)
    in_specs = (
        P(EP, None),
        P(),
        P(TP, None),
        P(TP, None),
        P(TP, None),
        P(TP, None),
        P(TP, None),
        P(),
        P(EP, TP),
        P(TP),
        P(EP, None),
        P(EP, None),
        P(EP, None, TP),
        P(EP, None, TP),
        P(EP, TP, None),
    )
    out_specs = (P(EP, None), P(EP, TP))
    return jax.shard_map(
        on_device, mesh=torus, in_specs=in_specs, out_specs=out_specs, check_vma=False
    )
```

```python
import math

import jax
import jax.numpy as jnp
from jax import lax
from jax.experimental import pallas as pl
from jax.experimental.pallas import tpu as pltpu
from jax.sharding import Mesh
from jax.sharding import PartitionSpec as P

EP = ("ep_0", "ep_1")
TP = ("tp_0", "tp_1")
Z, X, Y, C = 8, 4, 8, 2
N_EP, N_TP = Z * X, Y * C

EPSILON = 1e-06
CLAMP_LIMIT = 7.0
SILU_SHARPNESS = 1.702
LOG2E = math.log2(math.e)

D = 2048
HEAD = 64
ROWS = 256
HALF = ROWS // 2
TOK = 96
CAP = 16
SLOTS = N_EP * CAP
COLS = D // N_TP
GAIN_ROWS = 16
GRID_PIECES, ATT_PIECES, COLS_PIECES, SUM_PIECES = 4, 2, 2, 2
SUM_ROWS = SLOTS // SUM_PIECES

F32 = jnp.float32
BF16 = jnp.bfloat16
MESH = pl.DeviceIdType.MESH
NT = (((1,), (1,)), ((), ()))
TN = (((0,), (0,)), ((), ()))


def dot(a, b):
    return jnp.dot(a, b, preferred_element_type=F32)


def iota(shape, dim):
    return lax.broadcasted_iota(jnp.int32, shape, dim)


def split_two(value):
    high = value.astype(BF16)
    return high, (value - high.astype(F32)).astype(BF16)


def body(
    mix_rows, mix_gain, w_query, w_key, w_value, key_offset, w_out, out_gain, exp_rows, exp_gain,
    routes, route_weight, w_gate, w_up, w_down,
    mix_out, exp_out,
    gain_in, gain_out, offset, tokens, token_gain, route, route_scale,
    rows, wqkv, q_pad, kvg, acc, carry, far, drops, tri,
    picks, weight_hi, weight_lo, sent, grid, gains, wgu, gu, ssq, wd_own, wo_own, wo, wo_wide,
    part, pin, up_out, up_in, down_out, down_in,
    att, cols, result, returned,
    load_sem, disp_send, disp_recv, kva_send, kva_recv, kvb_send, kvb_recv,
    grid_send, grid_recv, gain_send, gain_recv, wo_send, wo_recv,
    pin_send, pin_recv, up_send, up_recv, down_send, down_recv,
    att_send, att_recv, cols_send, cols_recv, ret_send, ret_recv,
):
    z, x = lax.axis_index("ep_0"), lax.axis_index("ep_1")
    y, c = lax.axis_index("tp_0"), lax.axis_index("tp_1")
    ep, tp = z * X + x, y * C + c
    partner = {"tp_1": 1 - c}
    y_up, y_down = {"tp_0": lax.rem(y + 1, Y)}, {"tp_0": lax.rem(y + Y - 1, Y)}
    z_up, z_down = {"ep_0": lax.rem(z + 1, Z)}, {"ep_0": lax.rem(z + Z - 1, Z)}

    def ep_peer(distance):
        other = lax.rem(ep + distance, N_EP)
        return other, {"ep_0": other // X, "ep_1": lax.rem(other, X)}

    def tp_peer(distance):
        other = lax.rem(tp + distance, N_TP)
        return other, {"tp_0": other // C, "tp_1": lax.rem(other, C)}

    def x_peer(distance):
        return lax.rem(x + distance, X)

    def y_at(distance):
        return lax.rem(y + Y + distance, Y)

    def columns_of(other, width=COLS):
        return pl.ds(pl.multiple_of(other * width, width), width)

    def remote(src, dst, send_sem, recv_sem, device):
        return pltpu.make_async_remote_copy(
            src_ref=src, dst_ref=dst, send_sem=send_sem, recv_sem=recv_sem,
            device_id=device, device_id_type=MESH,
        )

    barrier = pltpu.get_barrier_semaphore()

    @pl.loop(1, N_EP)
    def _(distance):
        pl.semaphore_signal(barrier, 1, device_id=ep_peer(distance)[1], device_id_type=MESH)

    @pl.loop(1, N_TP)
    def _(distance):
        pl.semaphore_signal(barrier, 1, device_id=tp_peer(distance)[1], device_id_type=MESH)

    loads = {
        "route": (routes, route),
        "scale": (route_weight, route_scale),
        "tokens": (exp_rows, tokens),
        "token_gain": (exp_gain, token_gain),
        "gain_in": (mix_gain, gain_in),
        "rows": (mix_rows, rows),
        "query": (w_query, wqkv.at[pl.ds(0, HEAD)]),
        "key": (w_key, wqkv.at[pl.ds(2 * HEAD, HEAD)]),
        "value": (w_value, wqkv.at[pl.ds(3 * HEAD, HEAD)]),
        "w_out": (w_out, wo_own),
        "offset": (key_offset, offset),
        "gate": (w_gate.at[0], wgu.at[:, pl.ds(0, COLS)]),
        "up": (w_up.at[0], wgu.at[:, pl.ds(COLS, COLS)]),
        "down": (w_down.at[0], wd_own),
        "gain_out": (out_gain, gain_out),
    }
    loads = {
        name: pltpu.make_async_copy(a, b, load_sem.at[n])
        for n, (name, (a, b)) in enumerate(loads.items())
    }
    for load in loads.values():
        load.start()

    wqkv[pl.ds(HEAD, HEAD), :] = jnp.zeros((HEAD, D), BF16)
    tri[...] = jnp.where(
        (iota((256, 256), 1) >= HALF)
        | (lax.rem(iota((256, 256), 0), HALF) >= iota((256, 256), 1)), 1.0, 0.0,
    ).astype(BF16)

    for name in ("route", "scale", "tokens", "token_gain"):
        loads[name].wait()
    expert = iota((N_EP, TOK), 0)
    member = jnp.zeros((N_EP, TOK), F32)
    weight = jnp.zeros((N_EP, TOK), F32)
    for k in range(route.shape[0]):
        hit = route[k : k + 1, :] == expert
        member = member + jnp.where(hit, 1.0, 0.0)
        weight = weight + jnp.where(hit, route_scale[k : k + 1, :], 0.0)
    member = member.astype(BF16)
    earlier = jnp.where(iota((TOK, TOK), 0) < iota((TOK, TOK), 1), 1.0, 0.0).astype(BF16)
    before = dot(member, earlier).astype(BF16)
    spread = jnp.where(iota((SLOTS, N_EP), 0) // CAP == iota((SLOTS, N_EP), 1), 1.0, 0.0)
    spread = spread.astype(BF16)
    place = lax.rem(iota((SLOTS, TOK), 0), CAP).astype(F32)
    chosen = (dot(spread, member) > 0.5) & (dot(spread, before) == place)
    picks[...] = jnp.where(chosen, 1.0, 0.0).astype(BF16)
    high, low = split_two(weight)
    weight_hi[...] = jnp.where(chosen, dot(spread, high), 0.0).astype(BF16)
    weight_lo[...] = jnp.where(chosen, dot(spread, low), 0.0).astype(BF16)
    sent[...] = dot(picks[...], tokens[...]).astype(BF16)
    own_slots = pl.ds(pl.multiple_of(ep * CAP, CAP), CAP)
    grid[tp, own_slots, :] = sent[own_slots, :]
    gains[tp] = jnp.broadcast_to(token_gain[...], (GAIN_ROWS, COLS))

    loads["gain_in"].wait()
    loads["rows"].wait()
    gain = gain_in[...].astype(F32)
    gain = jnp.concatenate([gain[n : n + 1] for n in range(N_TP)], axis=1)

    @pl.loop(0, ROWS // 32)
    def _(n):
        at = pl.ds(pl.multiple_of(n * 32, 32), 32)
        numbers = rows[at, :].astype(F32)
        factor = lax.rsqrt(jnp.mean(numbers * numbers, axis=-1, keepdims=True) + EPSILON)
        rows[at, :] = (numbers * factor * gain).astype(BF16)

    for name in ("query", "key", "value"):
        loads[name].wait()
    projected = lax.dot_general(rows[...], wqkv[...], NT, preferred_element_type=F32).astype(BF16)
    q_pad[...] = projected[:, : 2 * HEAD]
    kvg[ep] = projected[:, 2 * HEAD :]
    loads["w_out"].wait()

    pl.semaphore_wait(barrier, N_EP - 1 + N_TP - 1)

    part_a, part_b = pl.ds(0, HALF), pl.ds(HALF, HALF)

    def send_a(slot, device):
        piece = kvg.at[slot, part_a]
        remote(piece, piece, kva_send, kva_recv.at[slot], device).start()

    def send_b(slot, device):
        piece = kvg.at[slot, part_b]
        remote(piece, piece, kvb_send, kvb_recv.at[slot], device).start()

    def wait_a(slot):
        piece = kvg.at[slot, part_a]
        remote(piece, piece, kva_send, kva_recv.at[slot], partner).wait_recv()

    def wait_b(slot):
        piece = kvg.at[slot, part_b]
        remote(piece, piece, kvb_send, kvb_recv.at[slot], partner).wait_recv()

    def send_b_across(slot):
        for distance in range(1, X):
            send_b(slot, {"ep_1": x_peer(distance)})

    @pl.loop(1, N_EP)
    def _(distance):
        other, device = ep_peer(distance)
        remote(
            sent.at[pl.ds(pl.multiple_of(other * CAP, CAP), CAP)],
            grid.at[tp, own_slots],
            disp_send, disp_recv, device,
        ).start()

    for distance in range(1, X):
        send_a(ep, {"ep_1": x_peer(distance)})
    send_b(ep, z_up)
    send_b(ep, z_down)
    send_a(ep, z_up)
    send_a(ep, z_down)
    send_b_across(ep)

    @pl.loop(1, N_TP)
    def _(distance):
        other, device = tp_peer(distance)
        remote(gains.at[tp], gains.at[tp], gain_send, gain_recv, device).start()
        remote(wo_own.at[:, columns_of(other)], wo.at[tp], wo_send, wo_recv, device).start()

    wo[tp] = wo_own[:, columns_of(tp)]

    for distance in range(1, X):
        slot = z * X + x_peer(distance)
        wait_a(slot)
        send_a(slot, z_up)
        send_a(slot, z_down)

    def attend(blocks, diagonal):
        count = len(blocks)
        scores = []
        for n, block in enumerate(blocks):
            shift = offset[:, pl.ds(pl.multiple_of(block * ROWS, ROWS), ROWS)] * LOG2E
            product = lax.dot_general(q_pad[...], kvg[block], NT, preferred_element_type=F32)
            product = product * (LOG2E / math.sqrt(HEAD)) + shift
            drop = jnp.maximum(jnp.log2(1.0 + jnp.exp2(jnp.minimum(product, 100.0))), product)
            if diagonal:
                visible = iota((ROWS, ROWS), 1) < iota((ROWS, ROWS), 0)
                drop = jnp.where(visible, drop, 0.0)
            scores.append(product)
            for half in range(2):
                high, low = split_two(drop[:, half * HALF : (half + 1) * HALF])
                at = pl.ds((2 * n + half) * ROWS, ROWS)
                drops[at, :HALF] = high
                drops[at, HALF:] = low
        totals = dot(drops[pl.ds(0, 2 * count * ROWS), :], tri[...])
        passed = jnp.zeros((ROWS, 128), F32)
        sums = jnp.zeros((ROWS, 128), F32)
        for n, block in enumerate(blocks):
            for half in (1, 0):
                at = slice(half * HALF, (half + 1) * HALF)
                total = totals[(2 * n + half) * ROWS : (2 * n + half + 1) * ROWS]
                weights = jnp.exp2(scores[n][:, at] - total[:, :HALF] - passed)
                if diagonal:
                    weights = jnp.where(visible[:, at], weights, 0.0)
                sums = sums + dot(weights.astype(BF16), kvg[block, pl.ds(half * HALF, HALF)])
                passed = passed + total[:, HALF:]
        return sums, passed

    def attend_near(blocks):
        sums, passed = attend(blocks, False)
        acc[...] += jnp.exp2(-carry[...]) * sums
        carry[...] += passed

    def row_blocks(row):
        return [row * X + X - 1 - n for n in range(X)]

    def near_row(back):
        @pl.when(z >= back)
        def _():
            attend_near(row_blocks(z - back))

    def far_row(back):
        @pl.when(z >= back)
        def _():
            sums, passed = attend(row_blocks(z - back), False)
            far[...] = sums + jnp.exp2(-passed) * far[...]

    def ring(buffer, pieces, send_sem, recv_sem):
        size = buffer.shape[1] // pieces
        early = pieces // 2

        def copy(slot, piece, device):
            block = buffer.at[slot, pl.ds(piece * size, size)]
            return remote(block, block, send_sem, recv_sem.at[slot, piece], device)

        def start():
            for piece in range(pieces):
                for device in (y_up, y_down, partner):
                    copy(tp, piece, device).start()

        def step(k):
            above, below = y_at(-k) * C + c, y_at(k) * C + c
            for piece in range(pieces):
                for slot, device, turn in ((above, y_up, True), (below, y_down, False)):
                    chosen = turn == (piece < early)
                    if k < Y // 2 or chosen:
                        copy(slot, piece, partner).wait_recv()
                        if k < Y // 2 - 1 or (k == Y // 2 - 1 and chosen):
                            copy(slot, piece, device).start()
                        copy(slot, piece, partner).start()

        def handed(chip):
            for piece in range(pieces):
                copy(chip * C + 1 - c, piece, partner).wait_recv()

        def drain():
            blocks = buffer.at[pl.ds(0, N_TP - 1)]
            remote(blocks, blocks, send_sem, recv_sem.at[0, 0], partner).wait_send()

        return start, step, handed, drain

    grid_start, grid_step, grid_handed, grid_drain = ring(grid, GRID_PIECES, grid_send, grid_recv)
    att_start, att_step, att_handed, att_drain = ring(att, ATT_PIECES, att_send, att_recv)
    cols_start, cols_step, cols_handed, cols_drain = ring(cols, COLS_PIECES, cols_send, cols_recv)

    arrived = grid.at[tp, pl.ds(0, SLOTS - CAP)]
    remote(arrived, arrived, disp_send, disp_recv, partner).wait_recv()
    grid_start()

    loads["offset"].wait()
    sums, passed = attend([ep], True)
    acc[...] = sums
    carry[...] = passed
    far[...] = jnp.zeros(far.shape, F32)
    for distance in range(1, X):
        wait_b(z * X + x_peer(distance))

    @pl.loop(0, x)
    def _(n):
        attend_near([ep - 1 - n])

    arrived = gains.at[pl.ds(0, N_TP - 1)]
    remote(arrived, arrived, gain_send, gain_recv, partner).wait_recv()
    loads["gate"].wait()
    loads["up"].wait()
    gu[...] = jnp.zeros(gu.shape, F32)
    ssq[...] = jnp.zeros(ssq.shape, F32)

    def gate_up(chip):
        scaled = []
        squares = ssq[...]
        for core in range(C):
            numbers = grid[chip * C + core].astype(F32)
            squares = squares + numbers * numbers
            scaled.append((numbers * gains[chip * C + core][:1].astype(F32)).astype(BF16))
        ssq[...] = squares
        gu[...] += dot(jnp.concatenate(scaled, axis=1), wgu[columns_of(chip, C * COLS), :])

    def kv_step(k):
        for distance in range(X):
            for row, device, turn in ((z + Z - k, z_up, True), (z + k, z_down, False)):
                slot = lax.rem(row, Z) * X + x_peer(distance)
                if k < Z // 2 or turn:
                    wait_a(slot)
                    if k < Z // 2 - 1 or (k == Z // 2 - 1 and turn):
                        send_a(slot, device)
        for row, device, turn in ((z + Z - k, z_up, True), (z + k, z_down, False)):
            slot = lax.rem(row, Z) * X + x
            if k < Z // 2 or turn:
                wait_b(slot)
                if k < Z // 2 - 1 or (k == Z // 2 - 1 and turn):
                    send_b(slot, device)
                send_b_across(slot)

    def kv_finish(row):
        for distance in range(1, X):
            wait_b(lax.rem(row, Z) * X + x_peer(distance))

    for k in range(1, 5):
        kv_step(k)
        grid_step(k)
        grid_handed(y_at(1 - k))
        gate_up(y_at(1 - k))
        if k > 1:
            grid_handed(y_at(k - 1))
            gate_up(y_at(k - 1))
            kv_finish(z + Z - k + 1)
            near_row(k - 1)
            kv_finish(z + k - 1)
            far_row(Z - k + 1)

    grid_handed(y_at(4))
    gate_up(y_at(4))
    factor = lax.rsqrt(jnp.sum(ssq[...], axis=1, keepdims=True) / D + EPSILON)
    gate_part = jnp.minimum(gu[:, :COLS] * factor, CLAMP_LIMIT)
    up_part = jnp.clip(gu[:, COLS:] * factor, -CLAMP_LIMIT, CLAMP_LIMIT)
    hidden = (up_part + 1.0) * (gate_part * jax.nn.sigmoid(SILU_SHARPNESS * gate_part))
    hidden = hidden.astype(BF16)
    loads["down"].wait()
    for distance in (4, -3, 3, -2, 2, -1, 1, 0):
        chip = y_at(distance)
        product = dot(hidden, wd_own[:, columns_of(chip, C * COLS)]).astype(BF16)
        for core in range(C):
            part[chip * C + core] = product[:, core * COLS : (core + 1) * COLS]
        remote(
            part.at[chip * C + 1 - c], pin.at[chip], pin_send, pin_recv.at[chip], partner
        ).start()

    kv_finish(z + Z - 4)
    near_row(4)
    acc[...] += jnp.exp2(-carry[...]) * far[...]
    first = pltpu.roll(acc[pl.ds(0, HALF), :], HEAD, 1)
    att[tp] = jnp.where(iota((HALF, 128), 1) < HEAD, first, acc[pl.ds(HALF, HALF), :]).astype(BF16)
    att_start()

    def own_sum(chip, piece):
        at = pl.ds(piece * SUM_ROWS, SUM_ROWS)
        return part[chip * C + c, at, :].astype(F32) + pin[chip, at, :].astype(F32)

    def wait_pin(chip):
        remote(part.at[chip], pin.at[chip], pin_send, pin_recv.at[chip], partner).wait_recv()

    ways = ((1, 4, y_up, up_out, up_in, up_send, up_recv), (-1, 3, y_down, down_out, down_in, down_send, down_recv))

    def sum_copy(way, hop, piece):
        _, _, device, out, into, send_sem, recv_sem = way
        at = pl.ds(piece * SUM_ROWS, SUM_ROWS)
        return remote(out.at[hop, at], into.at[hop, at], send_sem, recv_sem.at[hop, piece], device)

    def sum_step(hop):
        live = [way for way in ways if hop < way[1]]
        chips = [y_at(sign * (hops - hop)) for sign, hops, *_ in live]
        for chip in chips:
            wait_pin(chip)
        for piece in range(SUM_PIECES):
            at = pl.ds(piece * SUM_ROWS, SUM_ROWS)
            for way, chip in zip(live, chips):
                total = own_sum(chip, piece)
                if hop > 0:
                    sum_copy(way, hop - 1, piece).wait_recv()
                    total = total + way[4][hop - 1, at, :].astype(F32)
                way[3][hop, at, :] = total.astype(BF16)
                sum_copy(way, hop, piece).start()

    pieces = wo.at[pl.ds(0, N_TP - 1)]
    remote(pieces, pieces, wo_send, wo_recv, partner).wait_recv()
    for n in range(N_TP):
        zeros = jnp.zeros((HEAD, COLS), BF16)
        wo_wide[pl.ds(n * 128, HEAD), :] = jnp.concatenate([wo[n], zeros], axis=1)
        wo_wide[pl.ds(n * 128 + HEAD, HEAD), :] = jnp.concatenate([zeros, wo[n]], axis=1)

    for k in range(1, 5):
        sum_step(k - 1)
        att_step(k)
    for chip in range(Y):
        att_handed(chip)

    product = dot(jnp.concatenate([att[n] for n in range(N_TP)], axis=1), wo_wide[...])
    cols[tp, pl.ds(0, HALF), :] = product[:, :COLS].astype(BF16)
    cols[tp, pl.ds(HALF, HALF), :] = product[:, COLS:].astype(BF16)
    cols_start()

    wait_pin(y)
    for piece in range(SUM_PIECES):
        at = pl.ds(piece * SUM_ROWS, SUM_ROWS)
        total = own_sum(y, piece)
        for way in ways:
            sum_copy(way, way[1] - 1, piece).wait_recv()
            total = total + way[4][way[1] - 1, at, :].astype(F32)
        result[at, :] = total.astype(BF16)
    returned[own_slots, :] = result[own_slots, :]

    @pl.loop(1, N_EP)
    def _(distance):
        other, device = ep_peer(distance)
        remote(
            result.at[pl.ds(pl.multiple_of(other * CAP, CAP), CAP)],
            returned.at[own_slots],
            ret_send, ret_recv, device,
        ).start()

    for k in range(1, 5):
        cols_step(k)

    arrived = returned.at[pl.ds(0, SLOTS - CAP)]
    remote(arrived, arrived, ret_send, ret_recv, partner).wait_recv()
    total = lax.dot_general(weight_hi[...], returned[...], TN, preferred_element_type=F32)
    total += lax.dot_general(weight_lo[...], returned[...], TN, preferred_element_type=F32)
    exp_out[...] = total.astype(BF16)

    for chip in range(Y):
        cols_handed(chip)
    loads["gain_out"].wait()
    squares = jnp.zeros((ROWS, COLS), F32)
    for n in range(N_TP):
        numbers = cols[n].astype(F32)
        squares = squares + numbers * numbers
    factor = lax.rsqrt(jnp.sum(squares, axis=1, keepdims=True) / D + EPSILON)
    gain = gain_out[...].astype(F32)
    for n in range(N_TP):
        at = slice(n * COLS, (n + 1) * COLS)
        mix_out[:, at] = (cols[n].astype(F32) * factor * gain[n : n + 1]).astype(BF16)

    piece = kvg.at[pl.ds(0, N_EP - 1), part_a]
    remote(piece, piece, kva_send, kva_recv.at[0], partner).wait_send()
    remote(piece, piece, kvb_send, kvb_recv.at[0], partner).wait_send()
    piece = sent.at[pl.ds(0, SLOTS - CAP)]
    remote(piece, piece, disp_send, disp_recv, partner).wait_send()
    remote(piece, piece, ret_send, ret_recv, partner).wait_send()
    piece = gains.at[pl.ds(0, N_TP - 1)]
    remote(piece, piece, gain_send, gain_recv, partner).wait_send()
    piece = wo.at[pl.ds(0, N_TP - 1)]
    remote(piece, piece, wo_send, wo_recv, partner).wait_send()
    remote(pin, pin, pin_send, pin_recv.at[0], partner).wait_send()
    remote(up_in, up_in, up_send, up_recv.at[0, 0], partner).wait_send()
    remote(down_in, down_in, down_send, down_recv.at[0, 0], partner).wait_send()
    for drain in (grid_drain, att_drain, cols_drain):
        drain()


def on_device(*args):
    (mix_rows, mix_gain, w_query, w_key, w_value, key_offset, w_out, out_gain, exp_rows, exp_gain,
     routes, route_weight, w_gate, w_up, w_down) = args
    vmem, hbm = pl.BlockSpec(memory_space=pltpu.VMEM), pl.BlockSpec(memory_space=pl.ANY)
    dma = pltpu.SemaphoreType.DMA
    return pl.pallas_call(
        body,
        out_shape=(
            jax.ShapeDtypeStruct((ROWS, D), BF16),
            jax.ShapeDtypeStruct((TOK, COLS), BF16),
        ),
        in_specs=[hbm] * 15,
        out_specs=(vmem, vmem),
        scratch_shapes=[
            pltpu.VMEM((N_TP, COLS), BF16),
            pltpu.VMEM((N_TP, COLS), BF16),
            pltpu.VMEM((1, N_EP * ROWS), F32),
            pltpu.VMEM((TOK, COLS), BF16),
            pltpu.VMEM((1, COLS), BF16),
            pltpu.VMEM((4, TOK), jnp.int32),
            pltpu.VMEM((4, TOK), F32),
            pltpu.VMEM((ROWS, D), BF16),
            pltpu.VMEM((4 * HEAD, D), BF16),
            pltpu.VMEM((ROWS, 128), BF16),
            pltpu.VMEM((N_EP, ROWS, 128), BF16),
            pltpu.VMEM((ROWS, 128), F32),
            pltpu.VMEM((ROWS, 128), F32),
            pltpu.VMEM((ROWS, 128), F32),
            pltpu.VMEM((2 * X * ROWS, ROWS), BF16),
            pltpu.VMEM((256, 256), BF16),
            pltpu.VMEM((SLOTS, TOK), BF16),
            pltpu.VMEM((SLOTS, TOK), BF16),
            pltpu.VMEM((SLOTS, TOK), BF16),
            pltpu.VMEM((SLOTS, COLS), BF16),
            pltpu.VMEM((N_TP, SLOTS, COLS), BF16),
            pltpu.VMEM((N_TP, GAIN_ROWS, COLS), BF16),
            pltpu.VMEM((D, 2 * COLS), BF16),
            pltpu.VMEM((SLOTS, 2 * COLS), F32),
            pltpu.VMEM((SLOTS, COLS), F32),
            pltpu.VMEM((COLS, D), BF16),
            pltpu.VMEM((HEAD, D), BF16),
            pltpu.VMEM((N_TP, HEAD, COLS), BF16),
            pltpu.VMEM((N_TP * 128, 2 * COLS), BF16),
            pltpu.VMEM((N_TP, SLOTS, COLS), BF16),
            pltpu.VMEM((Y, SLOTS, COLS), BF16),
            pltpu.VMEM((4, SLOTS, COLS), BF16),
            pltpu.VMEM((4, SLOTS, COLS), BF16),
            pltpu.VMEM((3, SLOTS, COLS), BF16),
            pltpu.VMEM((3, SLOTS, COLS), BF16),
            pltpu.VMEM((N_TP, HALF, 128), BF16),
            pltpu.VMEM((N_TP, ROWS, COLS), BF16),
            pltpu.VMEM((SLOTS, COLS), BF16),
            pltpu.VMEM((SLOTS, COLS), BF16),
            dma((15,)),
            dma(()), dma(()),
            dma(()), dma((N_EP,)), dma(()), dma((N_EP,)),
            dma(()), dma((N_TP, GRID_PIECES)),
            dma(()), dma(()), dma(()), dma(()),
            dma(()), dma((Y,)),
            dma(()), dma((4, SUM_PIECES)), dma(()), dma((3, SUM_PIECES)),
            dma(()), dma((N_TP, ATT_PIECES)), dma(()), dma((N_TP, COLS_PIECES)),
            dma(()), dma(()),
        ],
        compiler_params=pltpu.CompilerParams(
            collective_id=0, has_side_effects=True, vmem_limit_bytes=60 * 1024 * 1024
        ),
    )(
        mix_rows, mix_gain.reshape(N_TP, COLS), w_query, w_key, w_value, key_offset, w_out,
        out_gain.reshape(N_TP, COLS), exp_rows, exp_gain.reshape(1, COLS), routes.T, route_weight.T,
        w_gate, w_up, w_down,
    )


def solution(mesh):
    torus = Mesh(mesh.devices.reshape(Z, X, Y, C), EP + TP)
    in_specs = (
        P(EP, None),
        P(),
        P(TP, None),
        P(TP, None),
        P(TP, None),
        P(TP, None),
        P(TP, None),
        P(),
        P(EP, TP),
        P(TP),
        P(EP, None),
        P(EP, None),
        P(EP, None, TP),
        P(EP, None, TP),
        P(EP, TP, None),
    )
    out_specs = (P(EP, None), P(EP, TP))
    return jax.shard_map(
        on_device, mesh=torus, in_specs=in_specs, out_specs=out_specs, check_vma=False
    )
```

```python
import math

import jax
import jax.numpy as jnp
from jax import lax
from jax.experimental import pallas as pl
from jax.experimental.pallas import tpu as pltpu
from jax.sharding import Mesh
from jax.sharding import PartitionSpec as P

EP = ("ep_0", "ep_1")
TP = ("tp_0", "tp_1")
Z, X, Y, C = 8, 4, 8, 2
N_EP, N_TP = Z * X, Y * C

EPSILON = 1e-06
CLAMP_LIMIT = 7.0
SILU_SHARPNESS = 1.702
LOG2E = math.log2(math.e)

D = 2048
HEAD = 64
ROWS = 256
HALF = ROWS // 2
TOK = 96
CAP = 16
SLOTS = N_EP * CAP
COLS = D // N_TP
GAIN_ROWS = 16
GRID_PIECES, ATT_PIECES, SUM_PIECES = 4, 2, 4
SUM_ROWS = SLOTS // SUM_PIECES

F32 = jnp.float32
BF16 = jnp.bfloat16
MESH = pl.DeviceIdType.MESH
NT = (((1,), (1,)), ((), ()))
TN = (((0,), (0,)), ((), ()))


def dot(a, b):
    return jnp.dot(a, b, preferred_element_type=F32)


def iota(shape, dim):
    return lax.broadcasted_iota(jnp.int32, shape, dim)


def split_two(value):
    high = value.astype(BF16)
    return high, (value - high.astype(F32)).astype(BF16)


def body(
    mix_rows, mix_gain, w_query, w_key, w_value, key_offset, w_out, out_gain, exp_rows, exp_gain,
    routes, route_weight, w_gate, w_up, w_down,
    mix_out, exp_out,
    gain_in, gain_out, offset, tokens, token_gain, route, route_scale,
    rows, wqkv, q_pad, kvg, acc, carry, far, drops, tri,
    picks, weight_hi, weight_lo, sent, grid, gains, wgu, gu, ssq, wd_own, wo_own, wide, wide_other, mixed, mixed_out,
    part, pin, up_out, up_in, down_out, down_in,
    att, result, returned, exp_sum,
    load_sem, out_sem, disp_send, disp_recv, kva_send, kva_recv, kvb_send, kvb_recv, kvc_recv,
    wida_send, wida_recv, widb_send, widb_recv, widc_recv, over_send, over_recv,
    grid_send, grid_recv, grid_hand, gain_send, gain_recv, wo_send, wo_recv,
    pin_send, pin_recv, up_send, up_recv, down_send, down_recv,
    att_send, att_recv, att_hand, ret_send, ret_recv,
):
    z, x = lax.axis_index("ep_0"), lax.axis_index("ep_1")
    y, c = lax.axis_index("tp_0"), lax.axis_index("tp_1")
    ep, tp = z * X + x, y * C + c
    partner = {"tp_1": 1 - c}
    y_up, y_down = {"tp_0": lax.rem(y + 1, Y)}, {"tp_0": lax.rem(y + Y - 1, Y)}
    z_up, z_down = {"ep_0": lax.rem(z + 1, Z)}, {"ep_0": lax.rem(z + Z - 1, Z)}

    def ep_peer(turn):
        other = lax.rem(ep + 1 + lax.rem(turn + N_EP // 2 - 3, N_EP - 1), N_EP)
        return other, {"ep_0": other // X, "ep_1": lax.rem(other, X)}

    def tp_peer(distance):
        other = lax.rem(tp + distance, N_TP)
        return other, {"tp_0": other // C, "tp_1": lax.rem(other, C)}

    def x_peer(distance):
        return lax.rem(x + distance, X)

    def y_at(distance):
        return lax.rem(y + Y + distance, Y)

    def columns_of(other, width=COLS):
        return pl.ds(pl.multiple_of(other * width, width), width)

    def remote(src, dst, send_sem, recv_sem, device):
        return pltpu.make_async_remote_copy(
            src_ref=src, dst_ref=dst, send_sem=send_sem, recv_sem=recv_sem,
            device_id=device, device_id_type=MESH,
        )

    barrier = pltpu.get_barrier_semaphore()

    @pl.loop(1, N_EP)
    def _(distance):
        pl.semaphore_signal(barrier, 1, device_id=ep_peer(distance)[1], device_id_type=MESH)

    @pl.loop(1, N_TP)
    def _(distance):
        pl.semaphore_signal(barrier, 1, device_id=tp_peer(distance)[1], device_id_type=MESH)

    loads = {
        "route": (routes, route),
        "scale": (route_weight, route_scale),
        "tokens": (exp_rows, tokens),
        "token_gain": (exp_gain, token_gain),
        "gain_in": (mix_gain, gain_in),
        "rows": (mix_rows, rows),
        "query": (w_query, wqkv.at[pl.ds(0, HEAD)]),
        "key": (w_key, wqkv.at[pl.ds(2 * HEAD, HEAD)]),
        "value": (w_value, wqkv.at[pl.ds(3 * HEAD, HEAD)]),
        "w_out": (w_out, wo_own),
        "offset": (key_offset, offset),
        "gate": (w_gate.at[0], wgu.at[:, pl.ds(0, COLS)]),
        "up": (w_up.at[0], wgu.at[:, pl.ds(COLS, COLS)]),
        "down": (w_down.at[0], wd_own),
        "gain_out": (out_gain, gain_out),
    }
    loads = {
        name: pltpu.make_async_copy(a, b, load_sem.at[n])
        for n, (name, (a, b)) in enumerate(loads.items())
    }
    for load in loads.values():
        load.start()

    wqkv[pl.ds(HEAD, HEAD), :] = jnp.zeros((HEAD, D), BF16)
    later = lax.rem(iota((2 * ROWS, ROWS), 0), ROWS) >= iota((2 * ROWS, ROWS), 1)
    tri[...] = jnp.where(later, 1.0, 0.0).astype(BF16)

    for name in ("route", "scale", "tokens", "token_gain"):
        loads[name].wait()
    expert = iota((N_EP, TOK), 0)
    member = jnp.zeros((N_EP, TOK), F32)
    weight = jnp.zeros((N_EP, TOK), F32)
    for k in range(route.shape[0]):
        hit = route[k : k + 1, :] == expert
        member = member + jnp.where(hit, 1.0, 0.0)
        weight = weight + jnp.where(hit, route_scale[k : k + 1, :], 0.0)
    member = member.astype(BF16)
    earlier = jnp.where(iota((TOK, TOK), 0) < iota((TOK, TOK), 1), 1.0, 0.0).astype(BF16)
    before = dot(member, earlier).astype(BF16)
    spread = jnp.where(iota((SLOTS, N_EP), 0) // CAP == iota((SLOTS, N_EP), 1), 1.0, 0.0)
    spread = spread.astype(BF16)
    place = lax.rem(iota((SLOTS, TOK), 0), CAP).astype(F32)
    chosen = (dot(spread, member) > 0.5) & (dot(spread, before) == place)
    picks[...] = jnp.where(chosen, 1.0, 0.0).astype(BF16)
    high, low = split_two(weight)
    weight_hi[...] = jnp.where(chosen, dot(spread, high), 0.0).astype(BF16)
    weight_lo[...] = jnp.where(chosen, dot(spread, low), 0.0).astype(BF16)
    sent[...] = dot(picks[...], tokens[...]).astype(BF16)
    own_slots = pl.ds(pl.multiple_of(ep * CAP, CAP), CAP)
    grid[tp, own_slots, :] = sent[own_slots, :]
    gains[tp] = jnp.broadcast_to(token_gain[...], (GAIN_ROWS, COLS))

    pl.semaphore_wait(barrier, N_EP - 1 + N_TP - 1)

    @pl.loop(1, N_EP)
    def _(distance):
        other, device = ep_peer(distance)
        remote(
            sent.at[pl.ds(pl.multiple_of(other * CAP, CAP), CAP)],
            grid.at[tp, own_slots],
            disp_send, disp_recv, device,
        ).start()

    loads["w_out"].wait()
    wide_rows = pl.ds(pl.multiple_of((z // 2) * 16, 16), 16)
    wide_slots = pl.ds(pl.multiple_of(tp * 16, 16), 16)

    def wide_tile(core):
        group = x * 4 + core * 2 + lax.rem(z, 2)
        return wo_own.at[wide_rows, columns_of(group)]

    @pl.loop(1, N_TP)
    def _(distance):
        other, device = tp_peer(distance)
        remote(gains.at[tp], gains.at[tp], gain_send, gain_recv, device).start()
        remote(
            wide_tile(lax.rem(other, C)), wide.at[ep, wide_slots], wo_send, wo_recv, device
        ).start()

    wide[ep, wide_slots, :] = wide_tile(c)[...]

    loads["gain_in"].wait()
    loads["rows"].wait()
    gain = gain_in[...].astype(F32)
    gain = jnp.concatenate([gain[n : n + 1] for n in range(N_TP)], axis=1)

    @pl.loop(0, ROWS // 32)
    def _(n):
        at = pl.ds(pl.multiple_of(n * 32, 32), 32)
        numbers = rows[at, :].astype(F32)
        factor = lax.rsqrt(jnp.mean(numbers * numbers, axis=-1, keepdims=True) + EPSILON)
        rows[at, :] = (numbers * factor * gain).astype(BF16)

    for name in ("query", "key", "value"):
        loads[name].wait()
    projected = lax.dot_general(rows[...], wqkv[...], NT, preferred_element_type=F32).astype(BF16)
    q_pad[...] = projected[:, : 2 * HEAD]
    kvg[ep] = projected[:, 2 * HEAD :]

    def plane(buffer, a_send, a_recv, b_send, b_recv, c_recv):
        def copy_a(slot, device):
            piece = buffer.at[slot, pl.ds(0, HALF)]
            return remote(piece, piece, a_send, a_recv.at[slot], device)

        def copy_b(slot, device):
            piece = buffer.at[slot, pl.ds(HALF, HALF)]
            return remote(piece, piece, b_send, b_recv.at[slot // X], device)

        def b_across(slot):
            piece = buffer.at[slot, pl.ds(HALF, HALF)]
            for distance in range(1, X):
                device = {"ep_1": x_peer(distance)}
                remote(piece, piece, b_send, c_recv.at[slot // X], device).start()

        def start():
            for distance in range(1, X):
                copy_a(ep, {"ep_1": x_peer(distance)}).start()
            copy_b(ep, z_up).start()
            copy_b(ep, z_down).start()
            copy_a(ep, z_up).start()
            copy_a(ep, z_down).start()
            b_across(ep)

        def across():
            for distance in range(1, X):
                slot = z * X + x_peer(distance)
                copy_a(slot, partner).wait_recv()
                copy_a(slot, z_up).start()
                copy_a(slot, z_down).start()

        def step(k, distance):
            for row, device, turn in ((z + Z - k, z_up, True), (z + k, z_down, False)):
                slot = lax.rem(row, Z) * X + x_peer(distance)
                if k < Z // 2 or turn:
                    copy_a(slot, partner).wait_recv()
                    if k < Z // 2 - 1 or (k == Z // 2 - 1 and turn):
                        copy_a(slot, device).start()

        def step_b(k):
            for row, device, turn in ((z + Z - k, z_up, True), (z + k, z_down, False)):
                slot = lax.rem(row, Z) * X + x
                if k < Z // 2 or turn:
                    copy_b(slot, partner).wait_recv()
                    if k < Z // 2 - 1 or (k == Z // 2 - 1 and turn):
                        copy_b(slot, device).start()
                    b_across(slot)

        def finish(row):
            pieces = buffer.at[pl.ds(0, X - 1), pl.ds(HALF, HALF)]
            recv_sem = c_recv.at[lax.rem(row, Z)]
            remote(pieces, pieces, b_send, recv_sem, partner).wait_recv()

        def drain():
            piece = buffer.at[pl.ds(0, N_EP - 1), pl.ds(0, HALF)]
            remote(piece, piece, a_send, a_recv.at[0], partner).wait_send()
            remote(piece, piece, b_send, b_recv.at[0], partner).wait_send()

        return start, across, step, step_b, finish, drain

    kv_start, kv_across, kv_step, kv_step_b, kv_finish, kv_drain = plane(
        kvg, kva_send, kva_recv, kvb_send, kvb_recv, kvc_recv
    )
    wide_start, wide_across, wide_step, wide_step_b, wide_finish, wide_drain = plane(
        wide, wida_send, wida_recv, widb_send, widb_recv, widc_recv
    )

    kv_start()
    def attend(blocks, diagonal):
        count = len(blocks)
        scores = []
        for n, block in enumerate(blocks):
            shift = offset[:, pl.ds(pl.multiple_of(block * ROWS, ROWS), ROWS)] * LOG2E
            product = lax.dot_general(q_pad[...], kvg[block], NT, preferred_element_type=F32)
            product = product * (LOG2E / math.sqrt(HEAD)) + shift
            drop = jnp.maximum(LOG2E * jnp.log(1.0 + jnp.exp2(jnp.minimum(product, 100.0))), product)
            if diagonal:
                visible = iota((ROWS, ROWS), 1) < iota((ROWS, ROWS), 0)
                drop = jnp.where(visible, drop, 0.0)
            scores.append(product)
            high, low = split_two(drop)
            at = pl.ds(n * ROWS, ROWS)
            drops[at, :ROWS] = high
            drops[at, ROWS:] = low
        passed = jnp.zeros((ROWS, 1), F32)
        sums = jnp.zeros((ROWS, 128), F32)
        totals = dot(drops[pl.ds(0, count * ROWS), :], tri[...])
        for n, block in enumerate(blocks):
            total = totals[n * ROWS : (n + 1) * ROWS]
            weights = jnp.exp2(scores[n] - (total + passed))
            if diagonal:
                weights = jnp.where(visible, weights, 0.0)
            sums = sums + dot(weights.astype(BF16), kvg[block])
            passed = passed + total[:, :1]
        return sums, passed

    def attend_near(blocks):
        sums, passed = attend(blocks, False)
        acc[...] += jnp.exp2(-carry[...]) * sums
        carry[...] += passed

    def row_blocks(row):
        return [row * X + X - 1 - n for n in range(X)]

    def near_row(back):
        @pl.when(z >= back)
        def _():
            attend_near(row_blocks(z - back))

    def far_row(back):
        @pl.when(z >= back)
        def _():
            sums, passed = attend(row_blocks(z - back), False)
            far[...] = sums + jnp.exp2(-passed) * far[...]

    def ring(buffer, pieces, send_sem, recv_sem, hand_sem):
        size = buffer.shape[1] // pieces
        early = pieces // 2

        def copy(slot, piece, device):
            block = buffer.at[slot, pl.ds(piece * size, size)]
            return remote(block, block, send_sem, recv_sem.at[slot // C, piece], device)

        def hand(slot, piece):
            block = buffer.at[slot, pl.ds(piece * size, size)]
            remote(block, block, send_sem, hand_sem.at[slot // C], partner).start()

        def start():
            for piece in range(pieces):
                copy(tp, piece, y_up).start()
                copy(tp, piece, y_down).start()
                hand(tp, piece)

        def step(k, piece):
            above, below = y_at(-k) * C + c, y_at(k) * C + c
            for slot, device, turn in ((above, y_up, True), (below, y_down, False)):
                chosen = turn == (piece < early)
                if k < Y // 2 or chosen:
                    copy(slot, piece, partner).wait_recv()
                    if k < Y // 2 - 1 or (k == Y // 2 - 1 and chosen):
                        copy(slot, piece, device).start()
                    hand(slot, piece)

        def handed(chip):
            block = buffer.at[chip * C + 1 - c]
            remote(block, block, send_sem, hand_sem.at[chip], partner).wait_recv()

        def drain():
            blocks = buffer.at[pl.ds(0, N_TP - 1)]
            remote(blocks, blocks, send_sem, hand_sem.at[0], partner).wait_send()

        return start, step, handed, drain

    grid_start, grid_step, grid_handed, grid_drain = ring(
        grid, GRID_PIECES, grid_send, grid_recv, grid_hand
    )
    att_start, att_step, att_handed, att_drain = ring(
        att, ATT_PIECES, att_send, att_recv, att_hand
    )

    arrived = grid.at[tp, pl.ds(0, SLOTS - CAP)]
    remote(arrived, arrived, disp_send, disp_recv, partner).wait_recv()
    grid_start()
    kv_across()
    loads["offset"].wait()
    sums, passed = attend([ep], True)
    acc[...] = sums
    carry[...] = jnp.broadcast_to(passed, carry.shape)
    far[...] = jnp.zeros(far.shape, F32)
    kv_finish(z)

    @pl.loop(0, x)
    def _(n):
        attend_near([ep - 1 - n])

    arrived = gains.at[pl.ds(0, N_TP - 1)]
    remote(arrived, arrived, gain_send, gain_recv, partner).wait_recv()
    loads["gate"].wait()
    loads["up"].wait()
    gu[...] = jnp.zeros(gu.shape, F32)
    ssq[...] = jnp.zeros(ssq.shape, F32)

    def gate_up(chip):
        scaled = []
        squares = ssq[...]
        for core in range(C):
            numbers = grid[chip * C + core].astype(F32)
            squares = squares + numbers * numbers
            scaled.append((numbers * gains[chip * C + core][:1].astype(F32)).astype(BF16))
        ssq[...] = squares
        gu[...] += dot(jnp.concatenate(scaled, axis=1), wgu[columns_of(chip, C * COLS), :])

    for k in range(1, 5):
        for piece in range(GRID_PIECES):
            grid_step(k, piece)
            kv_step(k, piece)
        kv_step_b(k)
        grid_handed(y_at(1 - k))
        gate_up(y_at(1 - k))
        if k > 1:
            grid_handed(y_at(k - 1))
            gate_up(y_at(k - 1))
        if k == 2:
            kv_finish(z + Z - 1)
            near_row(1)
        if k == 3:
            kv_finish(z + Z - 2)
            near_row(2)
            kv_finish(z + 1)
            far_row(7)

    pieces = wide.at[ep, pl.ds(0, ROWS - 16)]
    remote(pieces, pieces, wo_send, wo_recv, partner).wait_recv()
    wide_start()
    grid_handed(y_at(4))
    gate_up(y_at(4))
    factor = lax.rsqrt(jnp.sum(ssq[...], axis=1, keepdims=True) / D + EPSILON)
    gate_part = jnp.minimum(gu[:, :COLS] * factor, CLAMP_LIMIT)
    up_part = jnp.clip(gu[:, COLS:] * factor, -CLAMP_LIMIT, CLAMP_LIMIT)
    hidden = (up_part + 1.0) * (gate_part * jax.nn.sigmoid(SILU_SHARPNESS * gate_part))
    hidden = hidden.astype(BF16)
    loads["down"].wait()
    def down(distance):
        chip = y_at(distance)
        product = dot(hidden, wd_own[:, columns_of(chip, C * COLS)]).astype(BF16)
        for core in range(C):
            part[chip * C + core] = product[:, core * COLS : (core + 1) * COLS]
        remote(
            part.at[chip * C + 1 - c], pin.at[chip], pin_send, pin_recv.at[chip], partner
        ).start()

    for distance in (4, 3, -3):
        down(distance)

    def own_sum(chip, piece):
        at = pl.ds(piece * SUM_ROWS, SUM_ROWS)
        return part[chip * C + c, at, :].astype(F32) + pin[chip, at, :].astype(F32)

    def wait_pin(chip):
        remote(part.at[chip], pin.at[chip], pin_send, pin_recv.at[chip], partner).wait_recv()

    ways = (
        (1, True, y_up, up_out, up_in, up_send, up_recv),
        (-1, False, y_down, down_out, down_in, down_send, down_recv),
    )
    seen = set()

    def hops_of(way, piece):
        return 4 if way[1] == (piece < SUM_PIECES // 2) else 3

    def sum_copy(way, hop, piece):
        _, _, device, out, into, send_sem, recv_sem = way
        at = pl.ds(piece * SUM_ROWS, SUM_ROWS)
        return remote(out.at[hop, at], into.at[hop, at], send_sem, recv_sem.at[hop, piece], device)

    def sum_step(hop, piece):
        at = pl.ds(piece * SUM_ROWS, SUM_ROWS)
        for way in ways:
            distance = hops_of(way, piece) - hop
            if distance > 0:
                distance = way[0] * distance if distance < 4 else 4
                if distance not in seen:
                    seen.add(distance)
                    wait_pin(y_at(distance))
                total = own_sum(y_at(distance), piece)
                if hop > 0:
                    sum_copy(way, hop - 1, piece).wait_recv()
                    total = total + way[4][hop - 1, at, :].astype(F32)
                way[3][hop, at, :] = total.astype(BF16)
                sum_copy(way, hop, piece).start()

    for piece in range(SUM_PIECES):
        sum_step(0, piece)
    wide_across()
    for distance in (2, -2, 1, -1, 0):
        down(distance)
    kv_finish(z + Z - 3)
    near_row(3)
    kv_finish(z + 2)
    far_row(6)

    def hand_over(row):
        wide_finish(row)
        block = pl.ds(pl.multiple_of(lax.rem(row, Z) * X, X), X)
        at = lax.rem(row, Z)
        remote(wide.at[block], wide_other.at[block], over_send, over_recv.at[at], partner).start()

    for piece in range(SUM_PIECES):
        sum_step(1, piece)
        wide_step(1, piece)
    wide_step_b(1)
    hand_over(z)
    kv_finish(z + 3)
    far_row(5)
    kv_finish(z + Z - 4)
    near_row(4)
    acc[...] += jnp.exp2(-carry[...]) * far[...]
    att[tp] = jnp.transpose(acc[...])[HEAD:].astype(BF16)
    att_start()
    for piece in range(SUM_PIECES):
        sum_step(2, piece)
        wide_step(2, piece)
    wide_step_b(2)
    hand_over(z + Z - 1)
    hand_over(z + 1)
    for piece in range(ATT_PIECES):
        att_step(1, piece)
    for piece in range(SUM_PIECES):
        sum_step(3, piece)
        wide_step(3, piece)
    wide_step_b(3)
    hand_over(z + Z - 2)
    hand_over(z + 2)
    for piece in range(ATT_PIECES):
        att_step(2, piece)
    wait_pin(y)
    for piece in range(SUM_PIECES):
        at = pl.ds(piece * SUM_ROWS, SUM_ROWS)
        total = own_sum(y, piece)
        for way in ways:
            hop = hops_of(way, piece) - 1
            sum_copy(way, hop, piece).wait_recv()
            total = total + way[4][hop, at, :].astype(F32)
        result[at, :] = total.astype(BF16)
    returned[own_slots, :] = result[own_slots, :]

    @pl.loop(1, N_EP)
    def _(distance):
        other, device = ep_peer(distance)
        remote(
            result.at[pl.ds(pl.multiple_of(other * CAP, CAP), CAP)],
            returned.at[own_slots],
            ret_send, ret_recv, device,
        ).start()

    for piece in range(X):
        wide_step(4, piece)
    wide_step_b(4)
    for piece in range(ATT_PIECES):
        att_step(3, piece)
    hand_over(z + Z - 3)
    hand_over(z + 3)
    for piece in range(ATT_PIECES):
        att_step(4, piece)
    hand_over(z + 4)
    for chip in range(Y):
        att_handed(chip)
    for row in range(Z):
        block = wide.at[pl.ds(row * X, X)]
        remote(block, block, over_send, over_recv.at[row], partner).wait_recv()

    left = jnp.concatenate(
        [att[:, pl.ds(16 * n, 16), :].reshape(ROWS, ROWS) for n in range(4)], axis=0
    )
    left = jnp.transpose(left)
    squares = jnp.zeros((ROWS, COLS), F32)

    def project_out(core, source):
        squares = jnp.zeros((ROWS, COLS), F32)
        for across in range(X):
            right = jnp.concatenate(
                [
                    jnp.concatenate([source[(2 * n + m) * X + across] for n in range(4)], axis=0)
                    for m in range(2)
                ],
                axis=1,
            )
            product = dot(left, right)
            mixed[:, columns_of(across * 2 + core, 2 * COLS)] = product
            for m in range(2):
                numbers = product[:, m * COLS : (m + 1) * COLS]
                squares = squares + numbers * numbers
        return squares

    squares = project_out(c, wide) + project_out(1 - c, wide_other)
    loads["gain_out"].wait()
    factor = lax.rsqrt(jnp.sum(squares, axis=1, keepdims=True) / D + EPSILON)
    gain = gain_out[...].astype(F32)
    mix_copies = []
    for n in range(N_TP):
        at = pl.ds(n * COLS, COLS)
        mixed_out[:, at] = (mixed[:, at] * factor * gain[n : n + 1]).astype(BF16)
        if n % 4 == 3:
            at = pl.ds((n - 3) * COLS, 4 * COLS)
            mix_copies.append(
                pltpu.make_async_copy(mixed_out.at[:, at], mix_out.at[:, at], out_sem.at[n // 4])
            )
            mix_copies[-1].start()

    arrived = returned.at[pl.ds(0, SLOTS - CAP)]
    remote(arrived, arrived, ret_send, ret_recv, partner).wait_recv()
    total = lax.dot_general(weight_hi[...], returned[...], TN, preferred_element_type=F32)
    total += lax.dot_general(weight_lo[...], returned[...], TN, preferred_element_type=F32)
    exp_sum[...] = total.astype(BF16)
    exp_copy = pltpu.make_async_copy(exp_sum, exp_out, out_sem.at[4])
    exp_copy.start()

    kv_drain()
    wide_drain()
    remote(wide, wide, over_send, over_recv.at[0], partner).wait_send()
    piece = sent.at[pl.ds(0, SLOTS - CAP)]
    remote(piece, piece, disp_send, disp_recv, partner).wait_send()
    remote(piece, piece, ret_send, ret_recv, partner).wait_send()
    piece = gains.at[pl.ds(0, N_TP - 1)]
    remote(piece, piece, gain_send, gain_recv, partner).wait_send()
    piece = wide.at[0, pl.ds(0, ROWS - 16)]
    remote(piece, piece, wo_send, wo_recv, partner).wait_send()
    remote(pin, pin, pin_send, pin_recv.at[0], partner).wait_send()
    for into, send_sem, recv_sem in ((up_in, up_send, up_recv), (down_in, down_send, down_recv)):
        for piece in (into.at[pl.ds(0, 3)], into.at[3, pl.ds(0, SLOTS // 2)]):
            remote(piece, piece, send_sem, recv_sem.at[0, 0], partner).wait_send()
    grid_drain()
    att_drain()
    for copy in (*mix_copies, exp_copy):
        copy.wait()


def on_device(*args):
    (mix_rows, mix_gain, w_query, w_key, w_value, key_offset, w_out, out_gain, exp_rows, exp_gain,
     routes, route_weight, w_gate, w_up, w_down) = args
    hbm = pl.BlockSpec(memory_space=pl.ANY)
    dma = pltpu.SemaphoreType.DMA
    return pl.pallas_call(
        body,
        out_shape=(
            jax.ShapeDtypeStruct((ROWS, D), BF16),
            jax.ShapeDtypeStruct((TOK, COLS), BF16),
        ),
        in_specs=[hbm] * 15,
        out_specs=(hbm, hbm),
        scratch_shapes=[
            pltpu.VMEM((N_TP, COLS), BF16),
            pltpu.VMEM((N_TP, COLS), BF16),
            pltpu.VMEM((1, N_EP * ROWS), F32),
            pltpu.VMEM((TOK, COLS), BF16),
            pltpu.VMEM((1, COLS), BF16),
            pltpu.VMEM((4, TOK), jnp.int32),
            pltpu.VMEM((4, TOK), F32),
            pltpu.VMEM((ROWS, D), BF16),
            pltpu.VMEM((4 * HEAD, D), BF16),
            pltpu.VMEM((ROWS, 128), BF16),
            pltpu.VMEM((N_EP, ROWS, 128), BF16),
            pltpu.VMEM((ROWS, 128), F32),
            pltpu.VMEM((ROWS, 128), F32),
            pltpu.VMEM((ROWS, 128), F32),
            pltpu.VMEM((X * ROWS, 2 * ROWS), BF16),
            pltpu.VMEM((2 * ROWS, ROWS), BF16),
            pltpu.VMEM((SLOTS, TOK), BF16),
            pltpu.VMEM((SLOTS, TOK), BF16),
            pltpu.VMEM((SLOTS, TOK), BF16),
            pltpu.VMEM((SLOTS, COLS), BF16),
            pltpu.VMEM((N_TP, SLOTS, COLS), BF16),
            pltpu.VMEM((N_TP, GAIN_ROWS, COLS), BF16),
            pltpu.VMEM((D, 2 * COLS), BF16),
            pltpu.VMEM((SLOTS, 2 * COLS), F32),
            pltpu.VMEM((SLOTS, COLS), F32),
            pltpu.VMEM((COLS, D), BF16),
            pltpu.VMEM((HEAD, D), BF16),
            pltpu.VMEM((N_EP, ROWS, 128), BF16),
            pltpu.VMEM((N_EP, ROWS, 128), BF16),
            pltpu.VMEM((ROWS, D), F32),
            pltpu.VMEM((ROWS, D), BF16),
            pltpu.VMEM((N_TP, SLOTS, COLS), BF16),
            pltpu.VMEM((Y, SLOTS, COLS), BF16),
            pltpu.VMEM((4, SLOTS, COLS), BF16),
            pltpu.VMEM((4, SLOTS, COLS), BF16),
            pltpu.VMEM((4, SLOTS, COLS), BF16),
            pltpu.VMEM((4, SLOTS, COLS), BF16),
            pltpu.VMEM((N_TP, HEAD, ROWS), BF16),
            pltpu.VMEM((SLOTS, COLS), BF16),
            pltpu.VMEM((SLOTS, COLS), BF16),
            pltpu.VMEM((TOK, COLS), BF16),
            dma((15,)), dma((5,)),
            dma(()), dma(()),
            dma(()), dma((N_EP,)), dma(()), dma((Z,)), dma((Z,)),
            dma(()), dma((N_EP,)), dma(()), dma((Z,)), dma((Z,)),
            dma(()), dma((Z,)),
            dma(()), dma((Y, GRID_PIECES)), dma((Y,)),
            dma(()), dma(()), dma(()), dma(()),
            dma(()), dma((Y,)),
            dma(()), dma((4, SUM_PIECES)), dma(()), dma((4, SUM_PIECES)),
            dma(()), dma((Y, ATT_PIECES)), dma((Y,)),
            dma(()), dma(()),
        ],
        compiler_params=pltpu.CompilerParams(
            collective_id=0, has_side_effects=True, vmem_limit_bytes=60 * 1024 * 1024
        ),
    )(
        mix_rows, mix_gain.reshape(N_TP, COLS), w_query, w_key, w_value, key_offset, w_out,
        out_gain.reshape(N_TP, COLS), exp_rows, exp_gain.reshape(1, COLS), routes.T, route_weight.T,
        w_gate, w_up, w_down,
    )


def solution(mesh):
    torus = Mesh(mesh.devices.reshape(Z, X, Y, C), EP + TP)
    in_specs = (
        P(EP, None),
        P(),
        P(TP, None),
        P(TP, None),
        P(TP, None),
        P(TP, None),
        P(TP, None),
        P(),
        P(EP, TP),
        P(TP),
        P(EP, None),
        P(EP, None),
        P(EP, None, TP),
        P(EP, None, TP),
        P(EP, TP, None),
    )
    out_specs = (P(EP, None), P(EP, TP))
    return jax.shard_map(
        on_device, mesh=torus, in_specs=in_specs, out_specs=out_specs, check_vma=False
    )
```

```python
import math

import jax
import jax.numpy as jnp
from jax import lax
from jax.experimental import pallas as pl
from jax.experimental.pallas import tpu as pltpu
from jax.sharding import Mesh
from jax.sharding import PartitionSpec as P

EP = ("ep_0", "ep_1")
TP = ("tp_0", "tp_1")
Z, X, Y, C = 8, 4, 8, 2
N_EP, N_TP = Z * X, Y * C

EPSILON = 1e-06
CLAMP_LIMIT = 7.0
SILU_SHARPNESS = 1.702
LOG2E = math.log2(math.e)

D = 2048
HEAD = 64
ROWS = 256
HALF = ROWS // 2
TOK = 96
CAP = 16
SLOTS = N_EP * CAP
COLS = D // N_TP
GAIN_ROWS = 16
GRID_PIECES, SUM_PIECES = 4, 4
SUM_ROWS = SLOTS // SUM_PIECES

F32 = jnp.float32
BF16 = jnp.bfloat16
MESH = pl.DeviceIdType.MESH
NT = (((1,), (1,)), ((), ()))
TN = (((0,), (0,)), ((), ()))


def dot(a, b):
    return jnp.dot(a, b, preferred_element_type=F32)


def iota(shape, dim):
    return lax.broadcasted_iota(jnp.int32, shape, dim)


def split_two(value):
    high = value.astype(BF16)
    return high, (value - high.astype(F32)).astype(BF16)


def body(
    mix_rows, mix_gain, w_query, w_key, w_value, key_offset, w_out, out_gain, exp_rows, exp_gain,
    routes, route_weight, w_gate, w_up, w_down,
    mix_out, exp_out,
    gain_in, gain_out, offset, tokens, token_gain, route, route_scale,
    rows, wqkv, q_pad, q_help, kvg, acc, carry, far, far_out, far_in, drops, tri,
    picks, weight_hi, weight_lo, sent, grid, gains, wgu, gu, ssq, wd_own, wo_own, wide, wide_other, mixed, mixed_out,
    part, pin, up_out, up_in, down_out, down_in,
    att, result, returned, exp_sum,
    load_sem, out_sem, disp_send, disp_recv, kva_send, kva_recv, kvb_send, kvb_recv, kvc_recv,
    wida_send, wida_recv, widb_send, widb_recv, widc_recv, over_send, over_recv,
    grid_send, grid_recv, grid_hand, gain_send, gain_recv, wo_send, wo_recv,
    pin_send, pin_recv, up_send, up_recv, down_send, down_recv,
    att_send, att_recv, att_other, ret_send, ret_recv,
    q_send, q_recv, far_send, far_recv,
):
    z, x = lax.axis_index("ep_0"), lax.axis_index("ep_1")
    y, c = lax.axis_index("tp_0"), lax.axis_index("tp_1")
    ep, tp = z * X + x, y * C + c
    partner = {"tp_1": 1 - c}
    y_up, y_down = {"tp_0": lax.rem(y + 1, Y)}, {"tp_0": lax.rem(y + Y - 1, Y)}
    z_up, z_down = {"ep_0": lax.rem(z + 1, Z)}, {"ep_0": lax.rem(z + Z - 1, Z)}

    def ep_peer(turn):
        other = lax.rem(ep + 1 + lax.rem(turn + N_EP // 2 - 3, N_EP - 1), N_EP)
        return other, {"ep_0": other // X, "ep_1": lax.rem(other, X)}

    def tp_peer(distance):
        other = lax.rem(tp + distance, N_TP)
        return other, {"tp_0": other // C, "tp_1": lax.rem(other, C)}

    def x_peer(distance):
        return lax.rem(x + distance, X)

    def y_at(distance):
        return lax.rem(y + Y + distance, Y)

    def columns_of(other, width=COLS):
        return pl.ds(pl.multiple_of(other * width, width), width)

    def remote(src, dst, send_sem, recv_sem, device):
        return pltpu.make_async_remote_copy(
            src_ref=src, dst_ref=dst, send_sem=send_sem, recv_sem=recv_sem,
            device_id=device, device_id_type=MESH,
        )

    barrier = pltpu.get_barrier_semaphore()

    @pl.loop(1, N_EP, unroll=True)
    def _(distance):
        pl.semaphore_signal(barrier, 1, device_id=ep_peer(distance)[1], device_id_type=MESH)

    @pl.loop(1, N_TP, unroll=True)
    def _(distance):
        pl.semaphore_signal(barrier, 1, device_id=tp_peer(distance)[1], device_id_type=MESH)

    loads = {
        "route": (routes, route),
        "scale": (route_weight, route_scale),
        "tokens": (exp_rows, tokens),
        "token_gain": (exp_gain, token_gain),
        "gain_in": (mix_gain, gain_in),
        "rows": (mix_rows, rows),
        "query": (w_query, wqkv.at[pl.ds(0, HEAD)]),
        "key": (w_key, wqkv.at[pl.ds(2 * HEAD, HEAD)]),
        "value": (w_value, wqkv.at[pl.ds(3 * HEAD, HEAD)]),
        "w_out": (w_out, wo_own),
        "offset": (key_offset, offset),
        "gate": (w_gate.at[0], wgu.at[:, pl.ds(0, COLS)]),
        "up": (w_up.at[0], wgu.at[:, pl.ds(COLS, COLS)]),
        "down": (w_down.at[0], wd_own),
        "gain_out": (out_gain, gain_out),
    }
    loads = {
        name: pltpu.make_async_copy(a, b, load_sem.at[n])
        for n, (name, (a, b)) in enumerate(loads.items())
    }
    for load in loads.values():
        load.start()

    wqkv[pl.ds(HEAD, HEAD), :] = jnp.zeros((HEAD, D), BF16)
    tri[...] = jnp.where(iota((ROWS, ROWS), 0) > iota((ROWS, ROWS), 1), 1.0, 0.0).astype(BF16)

    for name in ("route", "scale", "tokens", "token_gain"):
        loads[name].wait()
    expert = iota((N_EP, TOK), 0)
    member = jnp.zeros((N_EP, TOK), F32)
    weight = jnp.zeros((N_EP, TOK), F32)
    for k in range(route.shape[0]):
        hit = route[k : k + 1, :] == expert
        member = member + jnp.where(hit, 1.0, 0.0)
        weight = weight + jnp.where(hit, route_scale[k : k + 1, :], 0.0)
    member = member.astype(BF16)
    earlier = jnp.where(iota((TOK, TOK), 0) < iota((TOK, TOK), 1), 1.0, 0.0).astype(BF16)
    before = dot(member, earlier).astype(BF16)
    spread = jnp.where(iota((SLOTS, N_EP), 0) // CAP == iota((SLOTS, N_EP), 1), 1.0, 0.0)
    spread = spread.astype(BF16)
    place = lax.rem(iota((SLOTS, TOK), 0), CAP).astype(F32)
    chosen = (dot(spread, member) > 0.5) & (dot(spread, before) == place)
    picks[...] = jnp.where(chosen, 1.0, 0.0).astype(BF16)
    high, low = split_two(weight)
    weight_hi[...] = jnp.where(chosen, dot(spread, high), 0.0).astype(BF16)
    weight_lo[...] = jnp.where(chosen, dot(spread, low), 0.0).astype(BF16)
    sent[...] = dot(picks[...], tokens[...]).astype(BF16)
    own_slots = pl.ds(pl.multiple_of(ep * CAP, CAP), CAP)
    grid[tp, own_slots, :] = sent[own_slots, :]
    gains[tp] = jnp.broadcast_to(token_gain[...], (GAIN_ROWS, COLS))

    loads["gain_in"].wait()
    loads["rows"].wait()
    gain = gain_in[...].astype(F32)
    gain = jnp.concatenate([gain[n : n + 1] for n in range(N_TP)], axis=1)

    @pl.loop(0, ROWS // 32)
    def _(n):
        at = pl.ds(pl.multiple_of(n * 32, 32), 32)
        numbers = rows[at, :].astype(F32)
        factor = lax.rsqrt(jnp.mean(numbers * numbers, axis=-1, keepdims=True) + EPSILON)
        rows[at, :] = (numbers * factor * gain).astype(BF16)

    for name in ("query", "key", "value"):
        loads[name].wait()
    projected = lax.dot_general(rows[...], wqkv[...], NT, preferred_element_type=F32).astype(BF16)
    q_pad[...] = projected[:, : 2 * HEAD]
    kvg[ep] = projected[:, 2 * HEAD :]

    pl.semaphore_wait(barrier, N_EP - 1 + N_TP - 1)

    @pl.loop(1, N_EP, unroll=True)
    def _(distance):
        other, device = ep_peer(distance)
        remote(
            sent.at[pl.ds(pl.multiple_of(other * CAP, CAP), CAP)],
            grid.at[tp, own_slots],
            disp_send, disp_recv, device,
        ).start()

    def plane(buffer, a_send, a_recv, b_send, b_recv, c_recv):
        def copy_a(slot, device):
            piece = buffer.at[slot, pl.ds(0, HALF)]
            return remote(piece, piece, a_send, a_recv.at[slot], device)

        def copy_b(slot, device):
            piece = buffer.at[slot, pl.ds(HALF, HALF)]
            return remote(piece, piece, b_send, b_recv.at[slot // X], device)

        def b_across(slot):
            piece = buffer.at[slot, pl.ds(HALF, HALF)]
            for distance in range(1, X):
                device = {"ep_1": x_peer(distance)}
                remote(piece, piece, b_send, c_recv.at[slot // X], device).start()

        def start():
            for distance in range(1, X):
                copy_a(ep, {"ep_1": x_peer(distance)}).start()
            copy_b(ep, z_up).start()
            copy_b(ep, z_down).start()
            copy_a(ep, z_up).start()
            copy_a(ep, z_down).start()
            b_across(ep)

        def across():
            for distance in range(1, X):
                slot = z * X + x_peer(distance)
                copy_a(slot, partner).wait_recv()
                copy_a(slot, z_up).start()
                copy_a(slot, z_down).start()

        def step(k, distance):
            for row, device, turn in ((z + Z - k, z_up, True), (z + k, z_down, False)):
                slot = lax.rem(row, Z) * X + x_peer(distance)
                if k < Z // 2 or turn:
                    copy_a(slot, partner).wait_recv()
                    if k < Z // 2 - 1 or (k == Z // 2 - 1 and turn):
                        copy_a(slot, device).start()

        def step_b(k):
            for row, device, turn in ((z + Z - k, z_up, True), (z + k, z_down, False)):
                slot = lax.rem(row, Z) * X + x
                if k < Z // 2 or turn:
                    copy_b(slot, partner).wait_recv()
                    if k < Z // 2 - 1 or (k == Z // 2 - 1 and turn):
                        copy_b(slot, device).start()
                    b_across(slot)

        def finish(row):
            pieces = buffer.at[pl.ds(0, X - 1), pl.ds(HALF, HALF)]
            recv_sem = c_recv.at[lax.rem(row, Z)]
            remote(pieces, pieces, b_send, recv_sem, partner).wait_recv()

        def drain():
            piece = buffer.at[pl.ds(0, N_EP - 1), pl.ds(0, HALF)]
            remote(piece, piece, a_send, a_recv.at[0], partner).wait_send()
            remote(piece, piece, b_send, b_recv.at[0], partner).wait_send()

        return start, across, step, step_b, finish, drain

    kv_start, kv_across, kv_step, kv_step_b, kv_finish, kv_drain = plane(
        kvg, kva_send, kva_recv, kvb_send, kvb_recv, kvc_recv
    )
    wide_start, wide_across, wide_step, wide_step_b, wide_finish, wide_drain = plane(
        wide, wida_send, wida_recv, widb_send, widb_recv, widc_recv
    )

    kv_start()
    across_z = {"ep_0": Z - 1 - z}

    @pl.when(z >= 5)
    def _():
        remote(q_pad, q_help, q_send, q_recv, across_z).start()

    loads["w_out"].wait()
    wide_rows = pl.ds(pl.multiple_of((z // 2) * 16, 16), 16)
    wide_slots = pl.ds(pl.multiple_of(tp * 16, 16), 16)

    def wide_tile(core):
        group = x * 4 + core * 2 + lax.rem(z, 2)
        return wo_own.at[wide_rows, columns_of(group)]

    @pl.loop(1, N_TP, unroll=True)
    def _(distance):
        other, device = tp_peer(distance)
        remote(gains.at[tp], gains.at[tp], gain_send, gain_recv, device).start()
        remote(
            wide_tile(lax.rem(other, C)), wide.at[ep, wide_slots], wo_send, wo_recv, device
        ).start()

    wide[ep, wide_slots, :] = wide_tile(c)[...]

    def attend(blocks, diagonal=False, query=q_pad):
        count = len(blocks)
        takes, firsts = [], []
        for n, block in enumerate(blocks):
            shift = offset[:, pl.ds(pl.multiple_of(block * ROWS, ROWS), ROWS)] * LOG2E
            scores = lax.dot_general(query[...], kvg[block], NT, preferred_element_type=F32)
            scores = scores * (LOG2E / math.sqrt(HEAD)) + shift
            drop = LOG2E * jnp.log(1.0 + jnp.exp2(jnp.minimum(scores, 100.0)))
            drop = jnp.maximum(drop, scores)
            takes.append(scores - drop)
            if diagonal:
                visible = iota((ROWS, ROWS), 1) < iota((ROWS, ROWS), 0)
                drop = jnp.where(visible, drop, 0.0)
            firsts.append(drop[:, :1])
            drops[pl.ds(n * ROWS, ROWS), :] = drop.astype(BF16)
        passed = jnp.zeros((ROWS, 1), F32)
        sums = jnp.zeros((ROWS, 128), F32)
        totals = dot(drops[pl.ds(0, count * ROWS), :], tri[...])
        for n, block in enumerate(blocks):
            total = totals[n * ROWS : (n + 1) * ROWS]
            weights = jnp.exp2(takes[n] - (total + passed))
            if diagonal:
                weights = jnp.where(visible, weights, 0.0)
            sums = sums + dot(weights.astype(BF16), kvg[block])
            passed = passed + total[:, :1] + firsts[n]
        return sums, passed

    def attend_near(blocks):
        sums, passed = attend(blocks)
        acc[...] += jnp.exp2(-carry[...]) * sums
        carry[...] += passed

    def row_blocks(row):
        return [row * X + X - 1 - n for n in range(X)]

    def near_row(back):
        @pl.when(z >= back)
        def _():
            attend_near(row_blocks(z - back))

    def help_row(turn):
        @pl.when(z == turn)
        def _():
            remote(q_pad, q_help, q_send, q_recv, partner).wait_recv()

        @pl.when(z <= turn)
        def _():
            sums, passed = attend(row_blocks(turn - z), query=q_help)
            far[...] = sums + jnp.exp2(-passed) * far[...]

    def ring(buffer, pieces, send_sem, recv_sem, hand_sem):
        size = buffer.shape[1] // pieces
        early = pieces // 2

        def copy(slot, piece, device):
            block = buffer.at[slot, pl.ds(piece * size, size)]
            return remote(block, block, send_sem, recv_sem.at[slot // C, piece], device)

        def hand(slot, piece):
            block = buffer.at[slot, pl.ds(piece * size, size)]
            remote(block, block, send_sem, hand_sem.at[slot // C], partner).start()

        def start():
            for piece in range(pieces):
                copy(tp, piece, y_up).start()
                copy(tp, piece, y_down).start()
                hand(tp, piece)

        def step(k, piece):
            above, below = y_at(-k) * C + c, y_at(k) * C + c
            for slot, device, turn in ((above, y_up, True), (below, y_down, False)):
                chosen = turn == (piece < early)
                if k < Y // 2 or chosen:
                    copy(slot, piece, partner).wait_recv()
                    if k < Y // 2 - 1 or (k == Y // 2 - 1 and chosen):
                        copy(slot, piece, device).start()
                    hand(slot, piece)

        def handed(chip):
            block = buffer.at[chip * C + 1 - c]
            remote(block, block, send_sem, hand_sem.at[chip], partner).wait_recv()

        def drain():
            blocks = buffer.at[pl.ds(0, N_TP - 1)]
            remote(blocks, blocks, send_sem, hand_sem.at[0], partner).wait_send()

        return start, step, handed, drain

    grid_start, grid_step, grid_handed, grid_drain = ring(
        grid, GRID_PIECES, grid_send, grid_recv, grid_hand
    )

    def att_copy(distance, device):
        block = att.at[y_at(distance) * C + c]
        return remote(block, block, att_send, att_recv.at[y_at(distance)], device)

    def att_hand(distance):
        block = att.at[y_at(distance) * C + c]
        remote(block, block, att_send, att_other, partner).start()

    def att_start():
        for distance in (1, -1, 2, -2):
            att_copy(0, {"tp_0": y_at(distance)}).start()
        att_hand(0)

    def att_relay():
        att_copy(-2, partner).wait_recv()
        att_copy(-2, {"tp_0": y_at(2)}).start()
        att_copy(-2, {"tp_0": y_at(1)}).start()
        att_copy(2, partner).wait_recv()
        att_copy(2, {"tp_0": y_at(-1)}).start()
        for distance in (-2, 2):
            att_hand(distance)
        for distance in (-1, 1):
            att_copy(distance, partner).wait_recv()
            att_hand(distance)

    def att_rest():
        for distance in (-3, 3, 4):
            att_copy(distance, partner).wait_recv()
            att_hand(distance)

    loads["offset"].wait()
    sums, passed = attend([ep], True)
    acc[...] = sums
    carry[...] = jnp.broadcast_to(passed, carry.shape)
    far[...] = jnp.zeros(far.shape, F32)
    kv_step_b(1)
    kv_across()
    kv_finish(z)

    @pl.loop(0, x)
    def _(n):
        attend_near([ep - 1 - n])

    arrived = grid.at[tp, pl.ds(0, SLOTS - CAP)]
    remote(arrived, arrived, disp_send, disp_recv, partner).wait_recv()
    grid_start()
    kv_step_b(2)
    arrived = gains.at[pl.ds(0, N_TP - 1)]
    remote(arrived, arrived, gain_send, gain_recv, partner).wait_recv()
    loads["gate"].wait()
    loads["up"].wait()
    gu[...] = jnp.zeros(gu.shape, F32)
    ssq[...] = jnp.zeros(ssq.shape, F32)

    def gate_up(chip):
        scaled = []
        squares = ssq[...]
        for core in range(C):
            numbers = grid[chip * C + core].astype(F32)
            squares = squares + numbers * numbers
            scaled.append((numbers * gains[chip * C + core][:1].astype(F32)).astype(BF16))
        ssq[...] = squares
        gu[...] += dot(jnp.concatenate(scaled, axis=1), wgu[columns_of(chip, C * COLS), :])

    for k in range(1, 5):
        for piece in range(GRID_PIECES):
            grid_step(k, piece)
            kv_step(k, piece)
        if k < 3:
            kv_step_b(k + 2)
        grid_handed(y_at(1 - k))
        gate_up(y_at(1 - k))
        if k > 1:
            grid_handed(y_at(k - 1))
            gate_up(y_at(k - 1))
        if k == 1:
            kv_finish(z + Z - 1)
            near_row(1)
            help_row(0)
        if k == 2:
            kv_finish(z + Z - 2)
            kv_finish(z + 1)
            near_row(2)
            help_row(1)
        if k == 3:
            pieces = wide.at[ep, pl.ds(0, ROWS - 16)]
            remote(pieces, pieces, wo_send, wo_recv, partner).wait_recv()
            wide_start()

    grid_handed(y_at(4))
    gate_up(y_at(4))
    factor = lax.rsqrt(jnp.sum(ssq[...], axis=1, keepdims=True) / D + EPSILON)
    gate_part = jnp.minimum(gu[:, :COLS] * factor, CLAMP_LIMIT)
    up_part = jnp.clip(gu[:, COLS:] * factor, -CLAMP_LIMIT, CLAMP_LIMIT)
    hidden = (up_part + 1.0) * (gate_part * jax.nn.sigmoid(SILU_SHARPNESS * gate_part))
    hidden = hidden.astype(BF16)
    loads["down"].wait()
    def down(distance):
        chip = y_at(distance)
        product = dot(hidden, wd_own[:, columns_of(chip, C * COLS)]).astype(BF16)
        for core in range(C):
            part[chip * C + core] = product[:, core * COLS : (core + 1) * COLS]
        remote(
            part.at[chip * C + 1 - c], pin.at[chip], pin_send, pin_recv.at[chip], partner
        ).start()

    for distance in (4, 3, -3):
        down(distance)

    def own_sum(chip, piece):
        at = pl.ds(piece * SUM_ROWS, SUM_ROWS)
        return part[chip * C + c, at, :].astype(F32) + pin[chip, at, :].astype(F32)

    def wait_pin(chip):
        remote(part.at[chip], pin.at[chip], pin_send, pin_recv.at[chip], partner).wait_recv()

    ways = (
        (1, True, y_up, up_out, up_in, up_send, up_recv),
        (-1, False, y_down, down_out, down_in, down_send, down_recv),
    )
    seen = set()

    def hops_of(way, piece):
        return 4 if way[1] == (piece < SUM_PIECES // 2) else 3

    def sum_copy(way, hop, piece):
        _, _, device, out, into, send_sem, recv_sem = way
        at = pl.ds(piece * SUM_ROWS, SUM_ROWS)
        return remote(out.at[hop, at], into.at[hop, at], send_sem, recv_sem.at[hop, piece], device)

    def sum_step(hop, piece):
        at = pl.ds(piece * SUM_ROWS, SUM_ROWS)
        for way in ways:
            distance = hops_of(way, piece) - hop
            if distance > 0:
                distance = way[0] * distance if distance < 4 else 4
                if distance not in seen:
                    seen.add(distance)
                    wait_pin(y_at(distance))
                total = own_sum(y_at(distance), piece)
                if hop > 0:
                    sum_copy(way, hop - 1, piece).wait_recv()
                    total = total + way[4][hop - 1, at, :].astype(F32)
                way[3][hop, at, :] = total.astype(BF16)
                sum_copy(way, hop, piece).start()

    wide_across()
    wide_step_b(1)
    for piece in range(SUM_PIECES):
        sum_step(0, piece)
    for distance in (2, -2, 1, -1, 0):
        down(distance)
    kv_finish(z + Z - 3)
    kv_finish(z + 2)
    near_row(3)
    help_row(2)

    @pl.when(z <= 2)
    def _():
        far_out[...] = far[...].astype(BF16)
        remote(far_out, far_in, far_send, far_recv, across_z).start()


    def hand_over(row):
        wide_finish(row)
        block = pl.ds(pl.multiple_of(lax.rem(row, Z) * X, X), X)
        at = lax.rem(row, Z)
        remote(wide.at[block], wide_other.at[block], over_send, over_recv.at[at], partner).start()

    wide_step_b(2)
    for piece in range(SUM_PIECES):
        sum_step(1, piece)
        wide_step(1, piece)
    wide_step_b(3)
    hand_over(z)
    hand_over(z + Z - 1)
    hand_over(z + 1)
    kv_finish(z + 3)
    kv_finish(z + Z - 4)
    near_row(4)

    @pl.when(z >= 5)
    def _():
        remote(far_out, far_in, far_send, far_recv, across_z).wait_recv()
        acc[...] += jnp.exp2(-carry[...]) * far_in[...].astype(F32)

    att[tp] = jnp.transpose(acc[...])[HEAD:].astype(BF16)
    att_start()
    for piece in range(SUM_PIECES):
        sum_step(2, piece)
        wide_step(2, piece)
    wide_step_b(4)
    hand_over(z + Z - 2)
    hand_over(z + 2)
    att_relay()
    for piece in range(SUM_PIECES):
        sum_step(3, piece)
        wide_step(3, piece)
    hand_over(z + Z - 3)
    hand_over(z + 3)
    wait_pin(y)
    for piece in range(SUM_PIECES):
        at = pl.ds(piece * SUM_ROWS, SUM_ROWS)
        total = own_sum(y, piece)
        for way in ways:
            hop = hops_of(way, piece) - 1
            sum_copy(way, hop, piece).wait_recv()
            total = total + way[4][hop, at, :].astype(F32)
        result[at, :] = total.astype(BF16)
    returned[own_slots, :] = result[own_slots, :]

    @pl.loop(1, N_EP, unroll=True)
    def _(distance):
        other, device = ep_peer(distance)
        remote(
            result.at[pl.ds(pl.multiple_of(other * CAP, CAP), CAP)],
            returned.at[own_slots],
            ret_send, ret_recv, device,
        ).start()

    att_rest()
    for piece in range(X):
        wide_step(4, piece)
    hand_over(z + 4)
    blocks = att.at[pl.ds(0, Y)]
    remote(blocks, blocks, att_send, att_other, partner).wait_recv()
    for row in range(Z):
        block = wide.at[pl.ds(row * X, X)]
        remote(block, block, over_send, over_recv.at[row], partner).wait_recv()

    left = jnp.concatenate(
        [att[:, pl.ds(16 * n, 16), :].reshape(ROWS, ROWS) for n in range(4)], axis=0
    )
    left = jnp.transpose(left)
    squares = jnp.zeros((ROWS, COLS), F32)

    def project_out(core, source):
        squares = jnp.zeros((ROWS, COLS), F32)
        for across in range(X):
            right = jnp.concatenate(
                [
                    jnp.concatenate([source[(2 * n + m) * X + across] for n in range(4)], axis=0)
                    for m in range(2)
                ],
                axis=1,
            )
            product = dot(left, right)
            mixed[:, columns_of(across * 2 + core, 2 * COLS)] = product
            for m in range(2):
                numbers = product[:, m * COLS : (m + 1) * COLS]
                squares = squares + numbers * numbers
        return squares

    squares = project_out(c, wide) + project_out(1 - c, wide_other)
    loads["gain_out"].wait()
    factor = lax.rsqrt(jnp.sum(squares, axis=1, keepdims=True) / D + EPSILON)
    gain = gain_out[...].astype(F32)
    mix_copies = []
    for n in range(N_TP):
        at = pl.ds(n * COLS, COLS)
        mixed_out[:, at] = (mixed[:, at] * factor * gain[n : n + 1]).astype(BF16)
        if n % 4 == 3:
            at = pl.ds((n - 3) * COLS, 4 * COLS)
            mix_copies.append(
                pltpu.make_async_copy(mixed_out.at[:, at], mix_out.at[:, at], out_sem.at[n // 4])
            )
            mix_copies[-1].start()

    arrived = returned.at[pl.ds(0, SLOTS - CAP)]
    remote(arrived, arrived, ret_send, ret_recv, partner).wait_recv()
    total = lax.dot_general(weight_hi[...], returned[...], TN, preferred_element_type=F32)
    total += lax.dot_general(weight_lo[...], returned[...], TN, preferred_element_type=F32)
    exp_sum[...] = total.astype(BF16)
    exp_copy = pltpu.make_async_copy(exp_sum, exp_out, out_sem.at[4])
    exp_copy.start()

    kv_drain()

    @pl.when(z >= 5)
    def _():
        remote(q_pad, q_help, q_send, q_recv, across_z).wait_send()

    @pl.when(z <= 2)
    def _():
        remote(far_out, far_in, far_send, far_recv, across_z).wait_send()

    wide_drain()
    remote(wide, wide, over_send, over_recv.at[0], partner).wait_send()
    piece = sent.at[pl.ds(0, SLOTS - CAP)]
    remote(piece, piece, disp_send, disp_recv, partner).wait_send()
    remote(piece, piece, ret_send, ret_recv, partner).wait_send()
    piece = gains.at[pl.ds(0, N_TP - 1)]
    remote(piece, piece, gain_send, gain_recv, partner).wait_send()
    piece = wide.at[0, pl.ds(0, ROWS - 16)]
    remote(piece, piece, wo_send, wo_recv, partner).wait_send()
    remote(pin, pin, pin_send, pin_recv.at[0], partner).wait_send()
    for into, send_sem, recv_sem in ((up_in, up_send, up_recv), (down_in, down_send, down_recv)):
        for piece in (into.at[pl.ds(0, 3)], into.at[3, pl.ds(0, SLOTS // 2)]):
            remote(piece, piece, send_sem, recv_sem.at[0, 0], partner).wait_send()
    grid_drain()
    blocks = att.at[pl.ds(0, N_TP - 1)]
    remote(blocks, blocks, att_send, att_other, partner).wait_send()
    for copy in (*mix_copies, exp_copy):
        copy.wait()


def on_device(*args):
    (mix_rows, mix_gain, w_query, w_key, w_value, key_offset, w_out, out_gain, exp_rows, exp_gain,
     routes, route_weight, w_gate, w_up, w_down) = args
    hbm = pl.BlockSpec(memory_space=pl.ANY)
    dma = pltpu.SemaphoreType.DMA
    return pl.pallas_call(
        body,
        out_shape=(
            jax.ShapeDtypeStruct((ROWS, D), BF16),
            jax.ShapeDtypeStruct((TOK, COLS), BF16),
        ),
        in_specs=[hbm] * 15,
        out_specs=(hbm, hbm),
        scratch_shapes=[
            pltpu.VMEM((N_TP, COLS), BF16),
            pltpu.VMEM((N_TP, COLS), BF16),
            pltpu.VMEM((1, N_EP * ROWS), F32),
            pltpu.VMEM((TOK, COLS), BF16),
            pltpu.VMEM((1, COLS), BF16),
            pltpu.VMEM((4, TOK), jnp.int32),
            pltpu.VMEM((4, TOK), F32),
            pltpu.VMEM((ROWS, D), BF16),
            pltpu.VMEM((4 * HEAD, D), BF16),
            pltpu.VMEM((ROWS, 128), BF16),
            pltpu.VMEM((ROWS, 128), BF16),
            pltpu.VMEM((N_EP, ROWS, 128), BF16),
            pltpu.VMEM((ROWS, 128), F32),
            pltpu.VMEM((ROWS, 128), F32),
            pltpu.VMEM((ROWS, 128), F32),
            pltpu.VMEM((ROWS, 128), BF16),
            pltpu.VMEM((ROWS, 128), BF16),
            pltpu.VMEM((X * ROWS, ROWS), BF16),
            pltpu.VMEM((ROWS, ROWS), BF16),
            pltpu.VMEM((SLOTS, TOK), BF16),
            pltpu.VMEM((SLOTS, TOK), BF16),
            pltpu.VMEM((SLOTS, TOK), BF16),
            pltpu.VMEM((SLOTS, COLS), BF16),
            pltpu.VMEM((N_TP, SLOTS, COLS), BF16),
            pltpu.VMEM((N_TP, GAIN_ROWS, COLS), BF16),
            pltpu.VMEM((D, 2 * COLS), BF16),
            pltpu.VMEM((SLOTS, 2 * COLS), F32),
            pltpu.VMEM((SLOTS, COLS), F32),
            pltpu.VMEM((COLS, D), BF16),
            pltpu.VMEM((HEAD, D), BF16),
            pltpu.VMEM((N_EP, ROWS, 128), BF16),
            pltpu.VMEM((N_EP, ROWS, 128), BF16),
            pltpu.VMEM((ROWS, D), F32),
            pltpu.VMEM((ROWS, D), BF16),
            pltpu.VMEM((N_TP, SLOTS, COLS), BF16),
            pltpu.VMEM((Y, SLOTS, COLS), BF16),
            pltpu.VMEM((4, SLOTS, COLS), BF16),
            pltpu.VMEM((4, SLOTS, COLS), BF16),
            pltpu.VMEM((4, SLOTS, COLS), BF16),
            pltpu.VMEM((4, SLOTS, COLS), BF16),
            pltpu.VMEM((N_TP, HEAD, ROWS), BF16),
            pltpu.VMEM((SLOTS, COLS), BF16),
            pltpu.VMEM((SLOTS, COLS), BF16),
            pltpu.VMEM((TOK, COLS), BF16),
            dma((15,)), dma((5,)),
            dma(()), dma(()),
            dma(()), dma((N_EP,)), dma(()), dma((Z,)), dma((Z,)),
            dma(()), dma((N_EP,)), dma(()), dma((Z,)), dma((Z,)),
            dma(()), dma((Z,)),
            dma(()), dma((Y, GRID_PIECES)), dma((Y,)),
            dma(()), dma(()), dma(()), dma(()),
            dma(()), dma((Y,)),
            dma(()), dma((4, SUM_PIECES)), dma(()), dma((4, SUM_PIECES)),
            dma(()), dma((Y,)), dma(()),
            dma(()), dma(()),
            dma(()), dma(()), dma(()), dma(()),
        ],
        compiler_params=pltpu.CompilerParams(
            collective_id=0, has_side_effects=True, vmem_limit_bytes=60 * 1024 * 1024
        ),
    )(
        mix_rows, mix_gain.reshape(N_TP, COLS), w_query, w_key, w_value, key_offset, w_out,
        out_gain.reshape(N_TP, COLS), exp_rows, exp_gain.reshape(1, COLS), routes.T, route_weight.T,
        w_gate, w_up, w_down,
    )


def solution(mesh):
    torus = Mesh(mesh.devices.reshape(Z, X, Y, C), EP + TP)
    in_specs = (
        P(EP, None),
        P(),
        P(TP, None),
        P(TP, None),
        P(TP, None),
        P(TP, None),
        P(TP, None),
        P(),
        P(EP, TP),
        P(TP),
        P(EP, None),
        P(EP, None),
        P(EP, None, TP),
        P(EP, None, TP),
        P(EP, TP, None),
    )
    out_specs = (P(EP, None), P(EP, TP))
    return jax.shard_map(
        on_device, mesh=torus, in_specs=in_specs, out_specs=out_specs, check_vma=False
    )
```

```python
import math

import jax
import jax.numpy as jnp
from jax import lax
from jax.experimental import pallas as pl
from jax.experimental.pallas import tpu as pltpu
from jax.sharding import Mesh
from jax.sharding import PartitionSpec as P

EP = ("ep_0", "ep_1")
TP = ("tp_0", "tp_1")
Z, X, Y, C = 8, 4, 8, 2
N_EP, N_TP = Z * X, Y * C

EPSILON = 1e-06
CLAMP_LIMIT = 7.0
SILU_SHARPNESS = 1.702
LOG2E = math.log2(math.e)

D = 2048
HEAD = 64
ROWS = 256
HALF = ROWS // 2
TOK = 96
CAP = 16
SLOTS = N_EP * CAP
COLS = D // N_TP
GAIN_ROWS = 16
GRID_PIECES, SUM_PIECES = 4, 4
SUM_ROWS = SLOTS // SUM_PIECES

F32 = jnp.float32
BF16 = jnp.bfloat16
MESH = pl.DeviceIdType.MESH
NT = (((1,), (1,)), ((), ()))
TN = (((0,), (0,)), ((), ()))


def dot(a, b):
    return jnp.dot(a, b, preferred_element_type=F32)


def iota(shape, dim):
    return lax.broadcasted_iota(jnp.int32, shape, dim)


def split_two(value):
    high = value.astype(BF16)
    return high, (value - high.astype(F32)).astype(BF16)


def body(
    mix_rows, mix_gain, w_query, w_key, w_value, key_offset, w_out, out_gain, exp_rows, exp_gain,
    routes, route_weight, w_gate, w_up, w_down,
    mix_out, exp_out,
    gain_in, gain_out, offset, tokens, token_gain, route, route_scale,
    rows, wqkv, q_pad, q_help, kvg, acc, carry, far, far_out, far_in, drops, tri,
    picks, weight_hi, weight_lo, sent, grid, gains, wgu, gu, ssq, wd_own, wo_own, wide, wide_other, mixed, mixed_out,
    part, pin, up_out, up_in, down_out, down_in,
    att, result, returned, exp_sum,
    load_sem, out_sem, disp_send, disp_recv, kva_send, kva_recv, kvb_send, kvb_recv, kvc_recv,
    wida_send, wida_recv, widb_send, widb_recv, widc_recv, over_send, over_recv,
    grid_send, grid_recv, grid_hand, gain_send, gain_recv, wo_send, wo_recv,
    pin_send, pin_recv, up_send, up_recv, down_send, down_recv,
    att_send, att_recv, att_other, ret_send, ret_recv,
    q_send, q_recv, far_send, far_recv,
):
    z, x = lax.axis_index("ep_0"), lax.axis_index("ep_1")
    y, c = lax.axis_index("tp_0"), lax.axis_index("tp_1")
    ep, tp = z * X + x, y * C + c
    partner = {"tp_1": 1 - c}
    y_up, y_down = {"tp_0": lax.rem(y + 1, Y)}, {"tp_0": lax.rem(y + Y - 1, Y)}
    z_up, z_down = {"ep_0": lax.rem(z + 1, Z)}, {"ep_0": lax.rem(z + Z - 1, Z)}

    def ep_peer(turn):
        other = lax.rem(ep + 1 + lax.rem(turn + N_EP // 2 - 3, N_EP - 1), N_EP)
        return other, {"ep_0": other // X, "ep_1": lax.rem(other, X)}

    def tp_peer(distance):
        other = lax.rem(tp + distance, N_TP)
        return other, {"tp_0": other // C, "tp_1": lax.rem(other, C)}

    def x_peer(distance):
        return lax.rem(x + distance, X)

    def y_at(distance):
        return lax.rem(y + Y + distance, Y)

    def columns_of(other, width=COLS):
        return pl.ds(pl.multiple_of(other * width, width), width)

    def remote(src, dst, send_sem, recv_sem, device):
        return pltpu.make_async_remote_copy(
            src_ref=src, dst_ref=dst, send_sem=send_sem, recv_sem=recv_sem,
            device_id=device, device_id_type=MESH,
        )

    barrier = pltpu.get_barrier_semaphore()

    @pl.loop(1, N_EP, unroll=True)
    def _(distance):
        pl.semaphore_signal(barrier, 1, device_id=ep_peer(distance)[1], device_id_type=MESH)

    @pl.loop(1, N_TP, unroll=True)
    def _(distance):
        pl.semaphore_signal(barrier, 1, device_id=tp_peer(distance)[1], device_id_type=MESH)

    loads = {
        "route": (routes, route),
        "scale": (route_weight, route_scale),
        "tokens": (exp_rows, tokens),
        "token_gain": (exp_gain, token_gain),
        "gain_in": (mix_gain, gain_in),
        "rows": (mix_rows, rows),
        "query": (w_query, wqkv.at[pl.ds(0, HEAD)]),
        "key": (w_key, wqkv.at[pl.ds(2 * HEAD, HEAD)]),
        "value": (w_value, wqkv.at[pl.ds(3 * HEAD, HEAD)]),
        "w_out": (w_out, wo_own),
        "offset": (key_offset, offset),
        "gate": (w_gate.at[0], wgu.at[:, pl.ds(0, COLS)]),
        "up": (w_up.at[0], wgu.at[:, pl.ds(COLS, COLS)]),
        "down": (w_down.at[0], wd_own),
        "gain_out": (out_gain, gain_out),
    }
    loads = {
        name: pltpu.make_async_copy(a, b, load_sem.at[n])
        for n, (name, (a, b)) in enumerate(loads.items())
    }
    for load in loads.values():
        load.start()

    wqkv[pl.ds(HEAD, HEAD), :] = jnp.zeros((HEAD, D), BF16)
    tri[...] = jnp.where(iota((ROWS, ROWS), 0) > iota((ROWS, ROWS), 1), 1.0, 0.0).astype(BF16)

    for name in ("route", "scale", "tokens", "token_gain"):
        loads[name].wait()
    expert = iota((N_EP, TOK), 0)
    member = jnp.zeros((N_EP, TOK), F32)
    weight = jnp.zeros((N_EP, TOK), F32)
    for k in range(route.shape[0]):
        hit = route[k : k + 1, :] == expert
        member = member + jnp.where(hit, 1.0, 0.0)
        weight = weight + jnp.where(hit, route_scale[k : k + 1, :], 0.0)
    member = member.astype(BF16)
    earlier = jnp.where(iota((TOK, TOK), 0) < iota((TOK, TOK), 1), 1.0, 0.0).astype(BF16)
    before = dot(member, earlier).astype(BF16)
    spread = jnp.where(iota((SLOTS, N_EP), 0) // CAP == iota((SLOTS, N_EP), 1), 1.0, 0.0)
    spread = spread.astype(BF16)
    place = lax.rem(iota((SLOTS, TOK), 0), CAP).astype(F32)
    chosen = (dot(spread, member) > 0.5) & (dot(spread, before) == place)
    picks[...] = jnp.where(chosen, 1.0, 0.0).astype(BF16)
    high, low = split_two(weight)
    weight_hi[...] = jnp.where(chosen, dot(spread, high), 0.0).astype(BF16)
    weight_lo[...] = jnp.where(chosen, dot(spread, low), 0.0).astype(BF16)
    sent[...] = dot(picks[...], tokens[...]).astype(BF16)
    own_slots = pl.ds(pl.multiple_of(ep * CAP, CAP), CAP)
    grid[tp, own_slots, :] = sent[own_slots, :]
    gains[tp] = jnp.broadcast_to(token_gain[...], (GAIN_ROWS, COLS))

    loads["gain_in"].wait()
    loads["rows"].wait()
    gain = gain_in[...].astype(F32)
    gain = jnp.concatenate([gain[n : n + 1] for n in range(N_TP)], axis=1)

    @pl.loop(0, ROWS // 32)
    def _(n):
        at = pl.ds(pl.multiple_of(n * 32, 32), 32)
        numbers = rows[at, :].astype(F32)
        factor = lax.rsqrt(jnp.mean(numbers * numbers, axis=-1, keepdims=True) + EPSILON)
        rows[at, :] = (numbers * factor * gain).astype(BF16)

    for name in ("query", "key", "value"):
        loads[name].wait()
    projected = lax.dot_general(rows[...], wqkv[...], NT, preferred_element_type=F32).astype(BF16)
    q_pad[...] = projected[:, : 2 * HEAD]
    kvg[ep] = projected[:, 2 * HEAD :]

    pl.semaphore_wait(barrier, N_EP - 1 + N_TP - 1)

    @pl.loop(1, N_EP, unroll=True)
    def _(distance):
        other, device = ep_peer(distance)
        remote(
            sent.at[pl.ds(pl.multiple_of(other * CAP, CAP), CAP)],
            grid.at[tp, own_slots],
            disp_send, disp_recv, device,
        ).start()

    def plane(buffer, a_send, a_recv, b_send, b_recv, c_recv):
        def copy_a(slot, device):
            piece = buffer.at[slot, pl.ds(0, HALF)]
            return remote(piece, piece, a_send, a_recv.at[slot], device)

        def copy_b(slot, device):
            piece = buffer.at[slot, pl.ds(HALF, HALF)]
            return remote(piece, piece, b_send, b_recv.at[slot // X], device)

        def b_across(slot):
            piece = buffer.at[slot, pl.ds(HALF, HALF)]
            for distance in range(1, X):
                device = {"ep_1": x_peer(distance)}
                remote(piece, piece, b_send, c_recv.at[slot // X], device).start()

        def start():
            for distance in range(1, X):
                copy_a(ep, {"ep_1": x_peer(distance)}).start()
            copy_b(ep, z_up).start()
            copy_b(ep, z_down).start()
            copy_a(ep, z_up).start()
            copy_a(ep, z_down).start()
            b_across(ep)

        def across():
            for distance in range(1, X):
                slot = z * X + x_peer(distance)
                copy_a(slot, partner).wait_recv()
                copy_a(slot, z_up).start()
                copy_a(slot, z_down).start()

        def step(k, distance):
            for row, device, turn in ((z + Z - k, z_up, True), (z + k, z_down, False)):
                slot = lax.rem(row, Z) * X + x_peer(distance)
                if k < Z // 2 or turn:
                    copy_a(slot, partner).wait_recv()
                    if k < Z // 2 - 1 or (k == Z // 2 - 1 and turn):
                        copy_a(slot, device).start()

        def step_b(k):
            for row, device, turn in ((z + Z - k, z_up, True), (z + k, z_down, False)):
                slot = lax.rem(row, Z) * X + x
                if k < Z // 2 or turn:
                    copy_b(slot, partner).wait_recv()
                    if k < Z // 2 - 1 or (k == Z // 2 - 1 and turn):
                        copy_b(slot, device).start()
                    b_across(slot)

        def finish(row):
            pieces = buffer.at[pl.ds(0, X - 1), pl.ds(HALF, HALF)]
            recv_sem = c_recv.at[lax.rem(row, Z)]
            remote(pieces, pieces, b_send, recv_sem, partner).wait_recv()

        def drain():
            piece = buffer.at[pl.ds(0, N_EP - 1), pl.ds(0, HALF)]
            remote(piece, piece, a_send, a_recv.at[0], partner).wait_send()
            remote(piece, piece, b_send, b_recv.at[0], partner).wait_send()

        return start, across, step, step_b, finish, drain

    kv_start, kv_across, kv_step, kv_step_b, kv_finish, kv_drain = plane(
        kvg, kva_send, kva_recv, kvb_send, kvb_recv, kvc_recv
    )
    wide_start, wide_across, wide_step, wide_step_b, wide_finish, wide_drain = plane(
        wide, wida_send, wida_recv, widb_send, widb_recv, widc_recv
    )

    kv_start()
    across_z = {"ep_0": Z - 1 - z}

    @pl.when(z >= 5)
    def _():
        remote(q_pad, q_help, q_send, q_recv, across_z).start()

    loads["w_out"].wait()
    wide_rows = pl.ds(pl.multiple_of((z // 2) * 16, 16), 16)
    wide_slots = pl.ds(pl.multiple_of(tp * 16, 16), 16)

    def wide_tile(core):
        group = x * 4 + core * 2 + lax.rem(z, 2)
        return wo_own.at[wide_rows, columns_of(group)]

    @pl.loop(1, N_TP, unroll=True)
    def _(distance):
        other, device = tp_peer(distance)
        remote(gains.at[tp], gains.at[tp], gain_send, gain_recv, device).start()
        remote(
            wide_tile(lax.rem(other, C)), wide.at[ep, wide_slots], wo_send, wo_recv, device
        ).start()

    wide[ep, wide_slots, :] = wide_tile(c)[...]

    def attend(blocks, diagonal=False, query=q_pad):
        count = len(blocks)
        takes, firsts = [], []
        for n, block in enumerate(blocks):
            shift = offset[:, pl.ds(pl.multiple_of(block * ROWS, ROWS), ROWS)] * LOG2E
            scores = lax.dot_general(query[...], kvg[block], NT, preferred_element_type=F32)
            scores = scores * (LOG2E / math.sqrt(HEAD)) + shift
            drop = LOG2E * jnp.log(1.0 + jnp.exp2(jnp.minimum(scores, 100.0)))
            drop = jnp.maximum(drop, scores)
            takes.append(scores - drop)
            if diagonal:
                visible = iota((ROWS, ROWS), 1) < iota((ROWS, ROWS), 0)
                drop = jnp.where(visible, drop, 0.0)
            firsts.append(drop[:, :1])
            drops[pl.ds(n * ROWS, ROWS), :] = drop.astype(BF16)
        passed = jnp.zeros((ROWS, 1), F32)
        sums = jnp.zeros((ROWS, 128), F32)
        totals = dot(drops[pl.ds(0, count * ROWS), :], tri[...])
        for n, block in enumerate(blocks):
            total = totals[n * ROWS : (n + 1) * ROWS]
            weights = jnp.exp2(takes[n] - (total + passed))
            if diagonal:
                weights = jnp.where(visible, weights, 0.0)
            sums = sums + dot(weights.astype(BF16), kvg[block])
            passed = passed + total[:, :1] + firsts[n]
        return sums, passed

    def attend_near(blocks):
        sums, passed = attend(blocks)
        acc[...] += jnp.exp2(-carry[...]) * sums
        carry[...] += passed

    def row_blocks(row):
        return [row * X + X - 1 - n for n in range(X)]

    def near_row(back):
        @pl.when(z >= back)
        def _():
            attend_near(row_blocks(z - back))

    def help_row(turn):
        @pl.when(z == turn)
        def _():
            remote(q_pad, q_help, q_send, q_recv, partner).wait_recv()

        @pl.when(z <= turn)
        def _():
            sums, passed = attend(row_blocks(turn - z), query=q_help)
            far[...] = sums + jnp.exp2(-passed) * far[...]

    def ring(buffer, pieces, send_sem, recv_sem, hand_sem):
        size = buffer.shape[1] // pieces
        early = pieces // 2

        def copy(slot, piece, device):
            block = buffer.at[slot, pl.ds(piece * size, size)]
            return remote(block, block, send_sem, recv_sem.at[slot // C, piece], device)

        def hand(slot, piece):
            block = buffer.at[slot, pl.ds(piece * size, size)]
            remote(block, block, send_sem, hand_sem.at[slot // C], partner).start()

        def start():
            for piece in range(pieces):
                copy(tp, piece, y_up).start()
                copy(tp, piece, y_down).start()
                hand(tp, piece)

        def step(k, piece):
            above, below = y_at(-k) * C + c, y_at(k) * C + c
            for slot, device, turn in ((above, y_up, True), (below, y_down, False)):
                chosen = turn == (piece < early)
                if k < Y // 2 or chosen:
                    copy(slot, piece, partner).wait_recv()
                    if k < Y // 2 - 1 or (k == Y // 2 - 1 and chosen):
                        copy(slot, piece, device).start()
                    hand(slot, piece)

        def handed(chip):
            block = buffer.at[chip * C + 1 - c]
            remote(block, block, send_sem, hand_sem.at[chip], partner).wait_recv()

        def drain():
            blocks = buffer.at[pl.ds(0, N_TP - 1)]
            remote(blocks, blocks, send_sem, hand_sem.at[0], partner).wait_send()

        return start, step, handed, drain

    grid_start, grid_step, grid_handed, grid_drain = ring(
        grid, GRID_PIECES, grid_send, grid_recv, grid_hand
    )

    def att_copy(distance, device):
        block = att.at[y_at(distance) * C + c]
        return remote(block, block, att_send, att_recv.at[y_at(distance)], device)

    def att_hand(distance):
        block = att.at[y_at(distance) * C + c]
        remote(block, block, att_send, att_other, partner).start()

    def att_start():
        for distance in (1, -1, 2, -2):
            att_copy(0, {"tp_0": y_at(distance)}).start()
        att_hand(0)

    def att_relay():
        att_copy(-2, partner).wait_recv()
        att_copy(-2, {"tp_0": y_at(2)}).start()
        att_copy(-2, {"tp_0": y_at(1)}).start()
        att_copy(2, partner).wait_recv()
        att_copy(2, {"tp_0": y_at(-1)}).start()
        for distance in (-2, 2):
            att_hand(distance)
        for distance in (-1, 1):
            att_copy(distance, partner).wait_recv()
            att_hand(distance)

    def att_rest():
        for distance in (-3, 3, 4):
            att_copy(distance, partner).wait_recv()
            att_hand(distance)

    loads["offset"].wait()
    sums, passed = attend([ep], True)
    acc[...] = sums
    carry[...] = jnp.broadcast_to(passed, carry.shape)
    far[...] = jnp.zeros(far.shape, F32)
    kv_step_b(1)
    kv_across()
    kv_finish(z)

    @pl.loop(0, x)
    def _(n):
        attend_near([ep - 1 - n])

    arrived = grid.at[tp, pl.ds(0, SLOTS - CAP)]
    remote(arrived, arrived, disp_send, disp_recv, partner).wait_recv()
    grid_start()
    arrived = gains.at[pl.ds(0, N_TP - 1)]
    remote(arrived, arrived, gain_send, gain_recv, partner).wait_recv()
    loads["gate"].wait()
    loads["up"].wait()
    gu[...] = jnp.zeros(gu.shape, F32)
    ssq[...] = jnp.zeros(ssq.shape, F32)

    def gate_up(chip):
        scaled = []
        squares = ssq[...]
        for core in range(C):
            numbers = grid[chip * C + core].astype(F32)
            squares = squares + numbers * numbers
            scaled.append((numbers * gains[chip * C + core][:1].astype(F32)).astype(BF16))
        ssq[...] = squares
        gu[...] += dot(jnp.concatenate(scaled, axis=1), wgu[columns_of(chip, C * COLS), :])

    for k in range(1, 5):
        for piece in range(GRID_PIECES):
            grid_step(k, piece)
            kv_step(k, piece)
        if k < 4:
            kv_step_b(k + 1)
        grid_handed(y_at(1 - k))
        gate_up(y_at(1 - k))
        if k > 1:
            grid_handed(y_at(k - 1))
            gate_up(y_at(k - 1))
        if k == 1:
            kv_finish(z + Z - 1)
            near_row(1)
            help_row(0)
        if k == 2:
            kv_finish(z + Z - 2)
            kv_finish(z + 1)
            near_row(2)
            help_row(1)
        if k == 3:
            pieces = wide.at[ep, pl.ds(0, ROWS - 16)]
            remote(pieces, pieces, wo_send, wo_recv, partner).wait_recv()
            wide_start()

    grid_handed(y_at(4))
    gate_up(y_at(4))
    factor = lax.rsqrt(jnp.sum(ssq[...], axis=1, keepdims=True) / D + EPSILON)
    gate_part = jnp.minimum(gu[:, :COLS] * factor, CLAMP_LIMIT)
    up_part = jnp.clip(gu[:, COLS:] * factor, -CLAMP_LIMIT, CLAMP_LIMIT)
    hidden = (up_part + 1.0) * (gate_part * jax.nn.sigmoid(SILU_SHARPNESS * gate_part))
    hidden = hidden.astype(BF16)
    loads["down"].wait()
    def down(distance):
        chip = y_at(distance)
        product = dot(hidden, wd_own[:, columns_of(chip, C * COLS)]).astype(BF16)
        for core in range(C):
            part[chip * C + core] = product[:, core * COLS : (core + 1) * COLS]
        remote(
            part.at[chip * C + 1 - c], pin.at[chip], pin_send, pin_recv.at[chip], partner
        ).start()

    for distance in (4, 3, -3):
        down(distance)

    def own_sum(chip, piece):
        at = pl.ds(piece * SUM_ROWS, SUM_ROWS)
        return part[chip * C + c, at, :].astype(F32) + pin[chip, at, :].astype(F32)

    def wait_pin(chip):
        remote(part.at[chip], pin.at[chip], pin_send, pin_recv.at[chip], partner).wait_recv()

    ways = (
        (1, True, y_up, up_out, up_in, up_send, up_recv),
        (-1, False, y_down, down_out, down_in, down_send, down_recv),
    )
    seen = set()

    def hops_of(way, piece):
        return 4 if way[1] == (piece < SUM_PIECES // 2) else 3

    def sum_copy(way, hop, piece):
        _, _, device, out, into, send_sem, recv_sem = way
        at = pl.ds(piece * SUM_ROWS, SUM_ROWS)
        return remote(out.at[hop, at], into.at[hop, at], send_sem, recv_sem.at[hop, piece], device)

    def sum_step(hop, piece):
        at = pl.ds(piece * SUM_ROWS, SUM_ROWS)
        for way in ways:
            distance = hops_of(way, piece) - hop
            if distance > 0:
                distance = way[0] * distance if distance < 4 else 4
                if distance not in seen:
                    seen.add(distance)
                    wait_pin(y_at(distance))
                total = own_sum(y_at(distance), piece)
                if hop > 0:
                    sum_copy(way, hop - 1, piece).wait_recv()
                    total = total + way[4][hop - 1, at, :].astype(F32)
                way[3][hop, at, :] = total.astype(BF16)
                sum_copy(way, hop, piece).start()

    wide_across()
    wide_step_b(1)
    for piece in range(SUM_PIECES):
        sum_step(0, piece)
    for distance in (2, -2, 1, -1, 0):
        down(distance)
    kv_finish(z + Z - 3)
    kv_finish(z + 2)
    near_row(3)
    help_row(2)

    @pl.when(z <= 2)
    def _():
        far_out[...] = far[...].astype(BF16)
        remote(far_out, far_in, far_send, far_recv, across_z).start()


    def hand_over(row):
        wide_finish(row)
        block = pl.ds(pl.multiple_of(lax.rem(row, Z) * X, X), X)
        at = lax.rem(row, Z)
        remote(wide.at[block], wide_other.at[block], over_send, over_recv.at[at], partner).start()

    for piece in range(SUM_PIECES):
        sum_step(1, piece)
        wide_step(1, piece)
    wide_step_b(2)
    hand_over(z)
    kv_finish(z + 3)
    kv_finish(z + Z - 4)
    near_row(4)
    def att_begin():
        @pl.when(z >= 5)
        def _():
            remote(far_out, far_in, far_send, far_recv, across_z).wait_recv()
            acc[...] += jnp.exp2(-carry[...]) * far_in[...].astype(F32)

        att[tp] = jnp.transpose(acc[...])[HEAD:].astype(BF16)
        att_start()

    for piece in range(SUM_PIECES):
        sum_step(2, piece)
        wide_step(2, piece)
        if piece == 1:
            att_begin()
    wide_step_b(3)
    hand_over(z + Z - 1)
    hand_over(z + 1)
    for piece in range(SUM_PIECES):
        sum_step(3, piece)
        wide_step(3, piece)
    att_relay()
    wide_step_b(4)
    hand_over(z + Z - 2)
    hand_over(z + 2)
    wait_pin(y)
    for piece in range(SUM_PIECES):
        at = pl.ds(piece * SUM_ROWS, SUM_ROWS)
        total = own_sum(y, piece)
        for way in ways:
            hop = hops_of(way, piece) - 1
            sum_copy(way, hop, piece).wait_recv()
            total = total + way[4][hop, at, :].astype(F32)
        result[at, :] = total.astype(BF16)
    returned[own_slots, :] = result[own_slots, :]

    @pl.loop(1, N_EP, unroll=True)
    def _(distance):
        other, device = ep_peer(distance)
        remote(
            result.at[pl.ds(pl.multiple_of(other * CAP, CAP), CAP)],
            returned.at[own_slots],
            ret_send, ret_recv, device,
        ).start()

    att_rest()
    for piece in range(X):
        wide_step(4, piece)
    hand_over(z + Z - 3)
    hand_over(z + 3)
    hand_over(z + 4)
    blocks = att.at[pl.ds(0, Y)]
    remote(blocks, blocks, att_send, att_other, partner).wait_recv()
    for row in range(Z):
        block = wide.at[pl.ds(row * X, X)]
        remote(block, block, over_send, over_recv.at[row], partner).wait_recv()

    left = jnp.concatenate(
        [att[:, pl.ds(16 * n, 16), :].reshape(ROWS, ROWS) for n in range(4)], axis=0
    )
    left = jnp.transpose(left)
    squares = jnp.zeros((ROWS, COLS), F32)

    def project_out(core, source):
        squares = jnp.zeros((ROWS, COLS), F32)
        for across in range(X):
            right = jnp.concatenate(
                [
                    jnp.concatenate([source[(2 * n + m) * X + across] for n in range(4)], axis=0)
                    for m in range(2)
                ],
                axis=1,
            )
            product = dot(left, right)
            mixed[:, columns_of(across * 2 + core, 2 * COLS)] = product
            for m in range(2):
                numbers = product[:, m * COLS : (m + 1) * COLS]
                squares = squares + numbers * numbers
        return squares

    squares = project_out(c, wide) + project_out(1 - c, wide_other)
    loads["gain_out"].wait()
    factor = lax.rsqrt(jnp.sum(squares, axis=1, keepdims=True) / D + EPSILON)
    gain = gain_out[...].astype(F32)
    mix_copies = []
    for n in range(N_TP):
        at = pl.ds(n * COLS, COLS)
        mixed_out[:, at] = (mixed[:, at] * factor * gain[n : n + 1]).astype(BF16)
        if n % 4 == 3:
            at = pl.ds((n - 3) * COLS, 4 * COLS)
            mix_copies.append(
                pltpu.make_async_copy(mixed_out.at[:, at], mix_out.at[:, at], out_sem.at[n // 4])
            )
            mix_copies[-1].start()

    arrived = returned.at[pl.ds(0, SLOTS - CAP)]
    remote(arrived, arrived, ret_send, ret_recv, partner).wait_recv()
    total = lax.dot_general(weight_hi[...], returned[...], TN, preferred_element_type=F32)
    total += lax.dot_general(weight_lo[...], returned[...], TN, preferred_element_type=F32)
    exp_sum[...] = total.astype(BF16)
    exp_copy = pltpu.make_async_copy(exp_sum, exp_out, out_sem.at[4])
    exp_copy.start()

    kv_drain()

    @pl.when(z >= 5)
    def _():
        remote(q_pad, q_help, q_send, q_recv, across_z).wait_send()

    @pl.when(z <= 2)
    def _():
        remote(far_out, far_in, far_send, far_recv, across_z).wait_send()

    wide_drain()
    remote(wide, wide, over_send, over_recv.at[0], partner).wait_send()
    piece = sent.at[pl.ds(0, SLOTS - CAP)]
    remote(piece, piece, disp_send, disp_recv, partner).wait_send()
    remote(piece, piece, ret_send, ret_recv, partner).wait_send()
    piece = gains.at[pl.ds(0, N_TP - 1)]
    remote(piece, piece, gain_send, gain_recv, partner).wait_send()
    piece = wide.at[0, pl.ds(0, ROWS - 16)]
    remote(piece, piece, wo_send, wo_recv, partner).wait_send()
    remote(pin, pin, pin_send, pin_recv.at[0], partner).wait_send()
    for into, send_sem, recv_sem in ((up_in, up_send, up_recv), (down_in, down_send, down_recv)):
        for piece in (into.at[pl.ds(0, 3)], into.at[3, pl.ds(0, SLOTS // 2)]):
            remote(piece, piece, send_sem, recv_sem.at[0, 0], partner).wait_send()
    grid_drain()
    blocks = att.at[pl.ds(0, N_TP - 1)]
    remote(blocks, blocks, att_send, att_other, partner).wait_send()
    for copy in (*mix_copies, exp_copy):
        copy.wait()


def on_device(*args):
    (mix_rows, mix_gain, w_query, w_key, w_value, key_offset, w_out, out_gain, exp_rows, exp_gain,
     routes, route_weight, w_gate, w_up, w_down) = args
    hbm = pl.BlockSpec(memory_space=pl.ANY)
    dma = pltpu.SemaphoreType.DMA
    return pl.pallas_call(
        body,
        out_shape=(
            jax.ShapeDtypeStruct((ROWS, D), BF16),
            jax.ShapeDtypeStruct((TOK, COLS), BF16),
        ),
        in_specs=[hbm] * 15,
        out_specs=(hbm, hbm),
        scratch_shapes=[
            pltpu.VMEM((N_TP, COLS), BF16),
            pltpu.VMEM((N_TP, COLS), BF16),
            pltpu.VMEM((1, N_EP * ROWS), F32),
            pltpu.VMEM((TOK, COLS), BF16),
            pltpu.VMEM((1, COLS), BF16),
            pltpu.VMEM((4, TOK), jnp.int32),
            pltpu.VMEM((4, TOK), F32),
            pltpu.VMEM((ROWS, D), BF16),
            pltpu.VMEM((4 * HEAD, D), BF16),
            pltpu.VMEM((ROWS, 128), BF16),
            pltpu.VMEM((ROWS, 128), BF16),
            pltpu.VMEM((N_EP, ROWS, 128), BF16),
            pltpu.VMEM((ROWS, 128), F32),
            pltpu.VMEM((ROWS, 128), F32),
            pltpu.VMEM((ROWS, 128), F32),
            pltpu.VMEM((ROWS, 128), BF16),
            pltpu.VMEM((ROWS, 128), BF16),
            pltpu.VMEM((X * ROWS, ROWS), BF16),
            pltpu.VMEM((ROWS, ROWS), BF16),
            pltpu.VMEM((SLOTS, TOK), BF16),
            pltpu.VMEM((SLOTS, TOK), BF16),
            pltpu.VMEM((SLOTS, TOK), BF16),
            pltpu.VMEM((SLOTS, COLS), BF16),
            pltpu.VMEM((N_TP, SLOTS, COLS), BF16),
            pltpu.VMEM((N_TP, GAIN_ROWS, COLS), BF16),
            pltpu.VMEM((D, 2 * COLS), BF16),
            pltpu.VMEM((SLOTS, 2 * COLS), F32),
            pltpu.VMEM((SLOTS, COLS), F32),
            pltpu.VMEM((COLS, D), BF16),
            pltpu.VMEM((HEAD, D), BF16),
            pltpu.VMEM((N_EP, ROWS, 128), BF16),
            pltpu.VMEM((N_EP, ROWS, 128), BF16),
            pltpu.VMEM((ROWS, D), F32),
            pltpu.VMEM((ROWS, D), BF16),
            pltpu.VMEM((N_TP, SLOTS, COLS), BF16),
            pltpu.VMEM((Y, SLOTS, COLS), BF16),
            pltpu.VMEM((4, SLOTS, COLS), BF16),
            pltpu.VMEM((4, SLOTS, COLS), BF16),
            pltpu.VMEM((4, SLOTS, COLS), BF16),
            pltpu.VMEM((4, SLOTS, COLS), BF16),
            pltpu.VMEM((N_TP, HEAD, ROWS), BF16),
            pltpu.VMEM((SLOTS, COLS), BF16),
            pltpu.VMEM((SLOTS, COLS), BF16),
            pltpu.VMEM((TOK, COLS), BF16),
            dma((15,)), dma((5,)),
            dma(()), dma(()),
            dma(()), dma((N_EP,)), dma(()), dma((Z,)), dma((Z,)),
            dma(()), dma((N_EP,)), dma(()), dma((Z,)), dma((Z,)),
            dma(()), dma((Z,)),
            dma(()), dma((Y, GRID_PIECES)), dma((Y,)),
            dma(()), dma(()), dma(()), dma(()),
            dma(()), dma((Y,)),
            dma(()), dma((4, SUM_PIECES)), dma(()), dma((4, SUM_PIECES)),
            dma(()), dma((Y,)), dma(()),
            dma(()), dma(()),
            dma(()), dma(()), dma(()), dma(()),
        ],
        compiler_params=pltpu.CompilerParams(
            collective_id=0, has_side_effects=True, vmem_limit_bytes=60 * 1024 * 1024
        ),
    )(
        mix_rows, mix_gain.reshape(N_TP, COLS), w_query, w_key, w_value, key_offset, w_out,
        out_gain.reshape(N_TP, COLS), exp_rows, exp_gain.reshape(1, COLS), routes.T, route_weight.T,
        w_gate, w_up, w_down,
    )


def solution(mesh):
    torus = Mesh(mesh.devices.reshape(Z, X, Y, C), EP + TP)
    in_specs = (
        P(EP, None),
        P(),
        P(TP, None),
        P(TP, None),
        P(TP, None),
        P(TP, None),
        P(TP, None),
        P(),
        P(EP, TP),
        P(TP),
        P(EP, None),
        P(EP, None),
        P(EP, None, TP),
        P(EP, None, TP),
        P(EP, TP, None),
    )
    out_specs = (P(EP, None), P(EP, TP))
    return jax.shard_map(
        on_device, mesh=torus, in_specs=in_specs, out_specs=out_specs, check_vma=False
    )
```
